32 devices in a mesh: sp: 16 (over z, y, x), tp: 2 (over core).
Axes of the slice: x: 2, y: 2, z: 4, core: 2. Of those that a mesh axis runs over, the one named last changes fastest.
Arguments:
- mid_rows: bfloat16 [2048, 2048], P(('sp', 'tp')), may hold values from -6 to 6
- cotangent: bfloat16 [2048, 2048], P(('sp', 'tp')), may hold values from -6 to 6
- route_experts: int32 [2048, 2], P(('sp', 'tp')), may hold values from 0 to 15, as said below
- route_weights: float32 [2048, 2], P(('sp', 'tp')), may hold values from 0.05 to 0.6
- gate_weight: bfloat16 [16, 2048, 1024], P('sp', None, 'tp'), may hold values from -0.125 to 0.125
- up_weight: bfloat16 [16, 2048, 1024], P('sp', None, 'tp'), may hold values from -0.125 to 0.125
- down_weight: bfloat16 [16, 1024, 2048], P('sp', 'tp'), may hold values from -0.1875 to 0.1875
- out_weight: bfloat16 [2048, 2048], P(None, 'tp'), may hold values from -0.125 to 0.125
- queries: bfloat16 [2048, 1024], P('sp', 'tp'), may hold values from -6 to 6
- key_rows: bfloat16 [2048, 1024], P('sp', 'tp'), may hold values from -6 to 6
- value_rows: bfloat16 [2048, 2048], P('sp', 'tp'), may hold values from -6 to 6
- log_decay: float32 [2048, 1024], P('sp', 'tp'), may hold values from -1 to 0
Outputs:
- gate_gradient: bfloat16 [16, 2048, 1024], P('sp', None, 'tp')
- up_gradient: bfloat16 [16, 2048, 1024], P('sp', None, 'tp')
- down_gradient: bfloat16 [16, 1024, 2048], P('sp', 'tp')
- out_gradient: float32 [2048, 2048], P('sp', 'tp')
- query_gradient: bfloat16 [2048, 1024], P('sp', 'tp')
- key_gradient: bfloat16 [2048, 1024], P('sp', 'tp')
- value_gradient: bfloat16 [2048, 2048], P('sp', 'tp')
- decay_gradient: float32 [2048, 1024], P('sp', 'tp')
The draws below stay inside these ranges and needn't reach their ends.
Inputs may be any that keep to these rules, and one draw needn't show every extreme that they name: `route_experts`: each row names two different experts of one group: both lie among the same 4 consecutive numbers starting at a multiple of 4. Among the rows of one device, no expert is named more than 16 times, and one expert exactly 16 times.
All inputs are finite; a program needn't handle non-finite values.
Results may differ from the reference program's by a relative error of at most 0.0058.
Values may be sent and summed in bfloat16 or wider, within the bound.
A program may use at most 192 MiB of HBM per device.

```python
import math
import jax
import jax.numpy as jnp
from jax import lax

D = 2048
HEADS = 8
DK = 128
DV = 256
KEY_CHANNELS = 1024
VW = 2048
DE = 1024
GROUPS = 4
BLOCK = 64
TOK_DEV = 128
SEQUENCE_TOKENS = 2048
ROWS = 64
EXPERTS = 16
CAP = 16


def route_block(block_key):
    per_group = EXPERTS // GROUPS
    half_rows = ROWS // 2
    first_key, second_key, third_key, fourth_key = jax.random.split(block_key, 4)
    token_position = jnp.arange(ROWS, dtype=jnp.int32)
    heavy = token_position < half_rows
    cut_points = jax.random.randint(fourth_key, (2,), 0, half_rows + 1).astype(jnp.int32)
    lower_cut = jnp.minimum(cut_points[0], cut_points[1])
    upper_cut = jnp.maximum(cut_points[0], cut_points[1])
    spare = token_position - half_rows
    other_group = jnp.where(spare < lower_cut, 1, jnp.where(spare < upper_cut, 2, 3)).astype(jnp.int32)
    other_start = jnp.where(other_group == 1, 0, jnp.where(other_group == 2, lower_cut, upper_cut)).astype(jnp.int32)
    group = jnp.where(heavy, 0, other_group).astype(jnp.int32)
    group_rank = jnp.where(heavy, token_position, spare - other_start).astype(jnp.int32)
    local_first = group_rank % per_group
    local_second = (group_rank + 1) % per_group
    group_order = jax.random.permutation(first_key, GROUPS).astype(jnp.int32)
    local_keys = jax.random.split(second_key, GROUPS)
    local_order = jax.vmap(jax.random.permutation, in_axes=(0, None))(local_keys, per_group).astype(jnp.int32)
    target = group_order[group]
    expert_first = target * per_group + local_order[group, local_first]
    expert_second = target * per_group + local_order[group, local_second]
    paired = jnp.stack([expert_first, expert_second], axis=1)
    shuffle = jax.random.permutation(third_key, ROWS)
    return paired[shuffle].astype(jnp.int32)


def draw_route_experts(key, part):
    block_total = SEQUENCE_TOKENS // ROWS
    block_keys = jax.random.split(jax.random.fold_in(key, 11), block_total)
    return jax.vmap(route_block)(block_keys).reshape(SEQUENCE_TOKENS, 2).astype(jnp.int32)


def draw_log_decay(key, part):
    random_subkeys = jax.random.split(jax.random.fold_in(key, 23), 7)
    fast_share = 0.5
    fast_channel = jax.random.bernoulli(random_subkeys[0], fast_share, (KEY_CHANNELS,))
    slow_rate = jnp.exp(jax.random.uniform(random_subkeys[1], (KEY_CHANNELS,), jnp.float32, jnp.log(0.1), 0.0)) * (0.5 / SEQUENCE_TOKENS)
    fast_rate = jax.random.uniform(random_subkeys[2], (KEY_CHANNELS,), jnp.float32, 0.01, 1.0 / 30.0)
    channel_decay_rate = jnp.where(fast_channel, fast_rate, slow_rate)
    device_multiplier = jnp.exp(jax.random.uniform(random_subkeys[3], (SEQUENCE_TOKENS // TOK_DEV,), jnp.float32, jnp.log(0.5), 0.0))
    device_multiplier = jnp.repeat(device_multiplier, TOK_DEV)
    random_noise = jax.random.uniform(random_subkeys[4], (SEQUENCE_TOKENS, KEY_CHANNELS), jnp.float32, 0.5, 1.5)
    spike_location = jax.random.randint(random_subkeys[5], (2,), 0, SEQUENCE_TOKENS)
    spike_magnitude = jax.random.uniform(random_subkeys[6], (2, KEY_CHANNELS), jnp.float32, jnp.log(0.5), jnp.log(0.8))
    token_position = jnp.arange(SEQUENCE_TOKENS)
    spike_value = jnp.where(token_position[:, None] == spike_location[0], spike_magnitude[0][None, :], 0.0)
    spike_value = spike_value + jnp.where(token_position[:, None] == spike_location[1], spike_magnitude[1][None, :], 0.0)
    return (spike_value - channel_decay_rate[None, :] * device_multiplier[:, None] * random_noise).astype(jnp.float32)


def spiked(values, key, source, target, blocks, factor):
    def block_of(dim):
        return (jnp.arange(values.shape[dim]) // (values.shape[dim] // blocks)).reshape((-1,) + (1,) * (values.ndim - 1 - dim))

    one_side = jax.random.permutation(key, blocks)[block_of(target)]
    other_side = (block_of(target) + blocks // 2) % blocks
    return jnp.where((block_of(source) == one_side) | (block_of(source) == other_side), factor * values, values)


def levels(stream_key, shape, cuts, smallest, high):
    def one(position, parts):
        draws = jax.random.uniform(jax.random.fold_in(jax.random.fold_in(stream_key, 6), position), (parts,), jnp.float32, smallest / len(cuts), high / len(cuts))
        return jnp.repeat(jnp.exp(draws), shape[position] // parts).reshape((-1,) + (1,) * (len(shape) - position - 1))

    gain = one(*cuts[0])
    for cut in cuts[1:]:
        gain = gain * one(*cut)
    return gain


def gaussian(stream_key, shape, spread, reach, cuts=(), kind=jnp.bfloat16):
    values = jax.random.normal(stream_key, shape, jnp.float32) * spread
    if len(cuts) > 0:
        values = levels(stream_key, shape, cuts, -0.22, 0.18) * values
    return jnp.clip(values, min=-reach, max=reach).astype(kind)


def heavy_noise(own_key, dims, scale, bound, cuts, heavy, held_as=jnp.bfloat16):
    result = scale * jax.random.normal(own_key, dims, jnp.float32)
    if cuts:
        result = result * levels(own_key, dims, cuts, -0.22, 0.18)
    return jnp.clip(spiked(result, jax.random.fold_in(own_key, 3), *heavy), -bound, bound).astype(held_as)


def setup_inputs(seed: int = 0) -> dict:
    arg_keys = jax.random.split(jax.random.key(seed), 13)
    return {
        "mid_rows": gaussian(arg_keys[0], (SEQUENCE_TOKENS, D), 1.0, 6.0, ((0, 32),)),
        "cotangent": heavy_noise(arg_keys[1], (SEQUENCE_TOKENS, D), 1.0, 6.0, ((0, 32),), (0, 1, 32, 2.75)),
        "route_experts": draw_route_experts(jax.random.fold_in(arg_keys[12], 71), 0),
        "route_weights": jnp.clip(jnp.exp(math.log(0.6) - 2.4849067 * jax.random.uniform(arg_keys[3], (SEQUENCE_TOKENS, 2), jnp.float32) ** levels(arg_keys[3], (SEQUENCE_TOKENS, 2), ((0, 32),), -0.2, 0.2)), 0.05, 0.6),
        "gate_weight": gaussian(arg_keys[4], (EXPERTS, D, DE), D ** -0.5, 0.125, ((0, 16), (2, 2))),
        "up_weight": gaussian(arg_keys[5], (EXPERTS, D, DE), D ** -0.5, 0.125, ((0, 16), (2, 2))),
        "down_weight": gaussian(arg_keys[6], (EXPERTS, DE, D), DE ** -0.5, 0.1875, ((0, 16), (1, 2))),
        "out_weight": gaussian(arg_keys[7], (D, VW), VW ** -0.5, 0.125, ((1, 2),)),
        "queries": gaussian(arg_keys[8], (SEQUENCE_TOKENS, KEY_CHANNELS), 1.0, 6.0, ((0, 16), (1, 2))),
        "key_rows": gaussian(arg_keys[9], (SEQUENCE_TOKENS, KEY_CHANNELS), 1.0, 6.0, ((0, 16), (1, 2))),
        "value_rows": gaussian(arg_keys[10], (SEQUENCE_TOKENS, VW), 1.0, 6.0, ((0, 16), (1, 2))),
        "log_decay": draw_log_decay(jax.random.fold_in(arg_keys[12], 71), 0),
    }


precise = lax.Precision.HIGHEST
epsilon = 1e-06
contract_rows = (((0,), (0,)), ((), ()))
contract_cols = (((1,), (1,)), ((), ()))

def silu_parts(pre_gate):
    gate_sigmoid = jax.nn.sigmoid(pre_gate)
    gate_swish = pre_gate * gate_sigmoid
    gate_slope = gate_sigmoid * (1.0 + pre_gate * (1.0 - gate_sigmoid))
    return (gate_swish, gate_slope)

def mixer_normed(query_float, key_float, value_float, decay_float):
    block_count = SEQUENCE_TOKENS // BLOCK
    query_blocks = query_float.reshape(block_count, BLOCK, HEADS, DK) * DK ** (-0.5)
    key_blocks = key_float.reshape(block_count, BLOCK, HEADS, DK)
    value_blocks = value_float.reshape(block_count, BLOCK, HEADS, DV)
    decay_blocks = decay_float.reshape(block_count, BLOCK, HEADS, DK)
    lower_mask = jnp.tril(jnp.ones((BLOCK, BLOCK), jnp.float32))

    def advance(carry_state, inputs):
        query_block, key_block, value_block, decay_block = inputs
        running_log = jnp.cumsum(decay_block, axis=0)
        block_log = running_log[-1]
        query_decayed = query_block * jnp.exp(running_log)
        key_inverse = key_block * jnp.exp(-running_log)
        key_to_end = key_block * jnp.exp(block_log[None] - running_log)
        scores = jnp.einsum('ihc,jhc->hij', query_decayed, key_inverse, precision=precise) * lower_mask
        raw_out = jnp.einsum('hij,jhv->ihv', scores, value_block, precision=precise)
        raw_out = raw_out + jnp.einsum('ihc,hcv->ihv', query_decayed, carry_state, precision=precise)
        new_state = jnp.exp(block_log)[:, :, None] * carry_state + jnp.einsum('jhc,jhv->hcv', key_to_end, value_block, precision=precise)
        return (new_state, raw_out)
    zero_state = jnp.zeros((HEADS, DK, DV), jnp.float32)
    final_state, raw_out = lax.scan(advance, zero_state, (query_blocks, key_blocks, value_blocks, decay_blocks))
    inverse_root = lax.rsqrt(lax.optimization_barrier(jnp.mean(raw_out * raw_out, axis=-1, keepdims=True)) + epsilon)
    return (raw_out * inverse_root).reshape(SEQUENCE_TOKENS, HEADS * DV)

def reference(mid_rows, cotangent, route_experts, route_weights, gate_weight, up_weight, down_weight, out_weight, queries, key_rows, value_rows, log_decay):
    senders = SEQUENCE_TOKENS // ROWS
    slots_total = senders * CAP
    sender_picks = route_experts.reshape(senders, 2 * ROWS)
    one_hot = (sender_picks[:, :, None] == jnp.arange(EXPERTS, dtype=jnp.int32)[None, None, :]).astype(jnp.int32)
    slot_rank = lax.optimization_barrier(jnp.sum((jnp.cumsum(one_hot, axis=1) - one_hot) * one_hot, axis=2))
    slot_index = (jnp.arange(senders, dtype=jnp.int32)[:, None] * CAP + slot_rank).reshape(-1).astype(jnp.int32)
    flat_expert = sender_picks.reshape(-1)
    table = jnp.full((EXPERTS, slots_total), -1, jnp.int32).at[flat_expert, slot_index].set(jnp.arange(2 * SEQUENCE_TOKENS, dtype=jnp.int32))
    flat_weight = route_weights.reshape(-1)
    half_width = DE // 2

    def one_expert(inputs):
        gate_expert, up_expert, down_expert, entries = inputs
        live_slot = entries >= 0
        entry_index = jnp.maximum(entries, 0)
        token_index = entry_index // 2
        rows_in = jnp.where(live_slot[:, None], mid_rows[token_index], jnp.zeros((), jnp.bfloat16))
        scaled = jnp.where(live_slot[:, None], flat_weight[entry_index][:, None] * cotangent[token_index].astype(jnp.float32), 0.0).astype(jnp.bfloat16)
        pre_gate = jnp.dot(rows_in, gate_expert, preferred_element_type=jnp.float32)
        pre_up = jnp.dot(rows_in, up_expert, preferred_element_type=jnp.float32)
        gate_swish, gate_slope = silu_parts(pre_gate)
        hidden = (gate_swish * pre_up).astype(jnp.bfloat16)
        back_hidden = lax.dot_general(scaled, down_expert, contract_cols, preferred_element_type=jnp.float32)
        back_gate = (back_hidden * pre_up * gate_slope).astype(jnp.bfloat16)
        back_up = (back_hidden * gate_swish).astype(jnp.bfloat16)
        gate_total = lax.dot_general(rows_in, back_gate, contract_rows, preferred_element_type=jnp.float32).astype(jnp.bfloat16)
        up_total = lax.dot_general(rows_in, back_up, contract_rows, preferred_element_type=jnp.float32).astype(jnp.bfloat16)
        down_total = lax.dot_general(hidden, scaled, contract_rows, preferred_element_type=jnp.float32).astype(jnp.bfloat16)
        first_half = lax.dot_general(back_gate[:, :half_width], gate_expert[:, :half_width], contract_cols, preferred_element_type=jnp.float32)
        first_half = first_half + lax.dot_general(back_up[:, :half_width], up_expert[:, :half_width], contract_cols, preferred_element_type=jnp.float32)
        second_half = lax.dot_general(back_gate[:, half_width:], gate_expert[:, half_width:], contract_cols, preferred_element_type=jnp.float32)
        second_half = second_half + lax.dot_general(back_up[:, half_width:], up_expert[:, half_width:], contract_cols, preferred_element_type=jnp.float32)
        first_round, second_round = lax.optimization_barrier((first_half.astype(jnp.bfloat16), second_half.astype(jnp.bfloat16)))
        expert_rows = (first_round.astype(jnp.float32) + second_round.astype(jnp.float32)).astype(jnp.bfloat16)
        return (gate_total, up_total, down_total, expert_rows)
    gate_total, up_total, down_total, expert_rows = lax.map(one_expert, (gate_weight, up_weight, down_weight, table))
    picked = expert_rows[flat_expert, slot_index].reshape(SEQUENCE_TOKENS, 2, D)
    token_back = (cotangent.astype(jnp.float32) + picked[:, 0].astype(jnp.float32) + picked[:, 1].astype(jnp.float32)).astype(jnp.bfloat16)
    normed, pullback = jax.vjp(mixer_normed, queries.astype(jnp.float32), key_rows.astype(jnp.float32), value_rows.astype(jnp.float32), log_decay)
    normed_rows = normed.astype(jnp.bfloat16)
    out_gradient = lax.dot_general(token_back, normed_rows, contract_rows, preferred_element_type=jnp.float32)
    back_normed = jnp.dot(token_back, out_weight, preferred_element_type=jnp.float32)
    query_back, key_back, value_back, decay_back = pullback(back_normed)
    return (gate_total, up_total, down_total, out_gradient, query_back.astype(jnp.bfloat16), key_back.astype(jnp.bfloat16), value_back.astype(jnp.bfloat16), decay_back)
```

```python
import functools

import jax
import jax.numpy as jnp
from jax import lax
from jax.experimental import pallas as pl
from jax.experimental.pallas import tpu as pltpu
from jax.sharding import PartitionSpec as P

DK = 128
DV = 256
BLOCK = 64
GROUPS = 4

MESH = pl.DeviceIdType.MESH
F32 = jnp.float32
BF16 = jnp.bfloat16
epsilon = 1e-06
NN = (((1,), (0,)), ((), ()))
NT = (((1,), (1,)), ((), ()))
TN = (((0,), (0,)), ((), ()))
VMEM = pltpu.VMEM


def mm(a, b, dims=NN):
    return lax.dot_general(a, b, dims, preferred_element_type=F32)


def split2(x):
    high = x.astype(BF16)
    return (high, (x - high.astype(F32)).astype(BF16))


def split3(x):
    high, _ = split2(x)
    rest = x - high.astype(F32)
    return (high,) + split2(rest)


def mm3(a, b, dims=NN):
    return mm(a[0], b[0], dims) + (mm(a[0], b[1], dims) + mm(a[1], b[0], dims))


def mm2l(a, b, dims=NN):
    return mm(a[0], b, dims) + mm(a[1], b, dims)


def mm2r(a, b, dims=NN):
    return mm(a, b[0], dims) + mm(a, b[1], dims)


def place():
    count = lax.axis_size("sp")
    plane = count // GROUPS
    mine = lax.axis_index("sp")
    return (count, plane, mine, mine // plane, lax.rem(mine, plane), lax.axis_index("tp"))


def loop(low, high, act):
    def turn(step, carry):
        act(step)
        return carry

    lax.fori_loop(low, high, turn, 0)


def signal(where):
    pl.semaphore_signal(
        pltpu.get_barrier_semaphore(), inc=1, device_id=where, device_id_type=MESH
    )


def greet_all():
    count, plane, mine, z, p, core = place()
    loop(1, count, lambda step: signal({"sp": lax.rem(mine + step, count)}))
    signal({"tp": 1 - core})


def greet_near():
    count, plane, mine, z, p, core = place()
    loop(1, plane, lambda step: signal({"sp": z * plane + lax.rem(p + step, plane)}))
    loop(1, GROUPS, lambda step: signal({"sp": lax.rem(z + step, GROUPS) * plane + p}))
    signal({"tp": 1 - core})


def met(total):
    pl.semaphore_wait(pltpu.get_barrier_semaphore(), total)


def send(source, target, send_sem, recv_sem, where):
    return pltpu.make_async_remote_copy(
        src_ref=source,
        dst_ref=target,
        send_sem=send_sem,
        recv_sem=recv_sem,
        device_id=where,
        device_id_type=MESH,
    )


def tri(size, lower, strict=False):
    row = lax.broadcasted_iota(jnp.int32, (size, size), 0)
    col = lax.broadcasted_iota(jnp.int32, (size, size), 1)
    if lower:
        return row > col if strict else row >= col
    return row <= col


def head_parts(rl, q, k, h, mid_row):
    cols = slice(h * DK, (h + 1) * DK)
    rl_h = rl[:, cols]
    mid = rl_h[mid_row : mid_row + 1]
    last = rl_h[rl_h.shape[0] - 1 :]
    qs = q[:, cols].astype(F32) * DK ** (-0.5)
    kf = k[:, cols].astype(F32)
    return (rl_h, mid, last, qs, kf)


def scatter_pieces(target, value, h):
    count, rows = target.shape[0], target.shape[1]
    cols = slice(h * DK, (h + 1) * DK)
    for j in range(count):
        target[j, :, cols] = value[j * rows : (j + 1) * rows].astype(target.dtype)


class Scan:
    def __init__(self, total, got, ready, out, decs, s1, r1, s2, r2, backward):
        self.refs = (total, got, ready, out, decs)
        self.sems = (s1, r1, s2, r2)
        self.backward = backward

    def first(self, step, there):
        total, got, ready, out, decs = self.refs
        count, plane, mine, z, p, core = place()
        ahead = lax.rem(mine + step, count)
        return send(
            total.at[ahead], got.at[there], self.sems[0].at[step], self.sems[1].at[step], {"sp": ahead}
        )

    def second(self, step, there):
        total, got, ready, out, decs = self.refs
        count, plane, mine, z, p, core = place()
        ahead = lax.rem(mine + step, count)
        return send(
            ready.at[ahead], out.at[there], self.sems[2].at[step], self.sems[3].at[step], {"sp": ahead}
        )

    def start(self):
        total, got, ready, out, decs = self.refs
        count, plane, mine, z, p, core = place()
        loop(1, count, lambda step: self.first(step, mine).start())
        got[mine] = total[mine]

    def middle(self):
        total, got, ready, out, decs = self.refs
        count, plane, mine, z, p, core = place()
        loop(1, count, lambda step: self.first(step, lax.rem(mine + count - step, count)).wait_recv())

        def turn(position, carry):
            index = count - 1 - position if self.backward else position
            ready[index] = carry.astype(ready.dtype)
            return carry * decs[index] + got[index].astype(F32)

        lax.fori_loop(0, count, turn, jnp.zeros(got.shape[1:], F32))
        loop(1, count, lambda step: self.second(step, mine).start())
        out[mine] = ready[mine]

    def finish(self):
        count, plane, mine, z, p, core = place()
        loop(1, count, lambda step: self.second(step, lax.rem(mine + count - step, count)).wait_recv())

    def settle(self):
        count, plane, mine, z, p, core = place()

        def act(step):
            self.first(step, mine).wait_send()
            self.second(step, mine).wait_send()

        loop(1, count, act)


def front_kernel(
    mid_ref, cot_ref, ex_ref, wt_ref, q_ref, k_ref, v_ref, ld_ref,
    rows_ref, meta_ref, pick_ref, decs_ref, inc_ref, normed_ref, normed_rows_ref, inv_ref, rl_ref, score_ref, total_ref,
    pack, pack_meta, zbuf, wide, piece, got, ready, dec_mine,
    zs_sem, zr_sem, xs_sem, xr_sem, fs_sem, fr_sem, l_sem, s1, r1, s2, r2, ds, dr,
):
    count, plane, mine, z, p, core = place()
    tokens = mid_ref.shape[0]
    cap = rows_ref.shape[4]
    gcap = plane * cap // 2
    greet_all()

    lane = lax.broadcasted_iota(jnp.int32, (tokens, 128), 1)
    e0, e1 = ex_ref[:, 0:1], ex_ref[:, 1:2]
    w0, w1 = wt_ref[:, 0:1], wt_ref[:, 1:2]
    hit0, hit1 = (e0 == lane), (e1 == lane)
    earlier = tri(tokens, True, True).astype(F32).astype(BF16)
    named = (hit0.astype(F32) + hit1.astype(F32)).astype(BF16)
    before = mm(earlier, named)
    rank0 = jnp.sum(jnp.where(hit0, before, 0.0), axis=1, keepdims=True)
    rank1 = jnp.sum(jnp.where(hit1, before, 0.0), axis=1, keepdims=True)
    member = ((e0 >= lane * plane) & (e0 < lane * plane + plane)).astype(F32)
    ahead_count = mm(earlier, member.astype(BF16))
    rank_group = jnp.sum(member * ahead_count, axis=1, keepdims=True)
    group = jnp.sum(member * lane.astype(F32), axis=1, keepdims=True)
    lane_f = lane.astype(F32)
    pick = (group * gcap + rank_group == lane_f).astype(F32).astype(BF16)
    pick_ref[...] = pick
    slot0 = (e0.astype(F32) - group * plane) * cap + rank0
    slot1 = (e1.astype(F32) - group * plane) * cap + rank1
    weights = jnp.where(slot0 == lane_f, w0, 0.0) + jnp.where(slot1 == lane_f, w1, 0.0)
    parts = split3(weights)
    packed_meta = mm(pick, parts[0], TN) + (mm(pick, parts[1], TN) + mm(pick, parts[2], TN))
    pack_meta[...] = packed_meta.reshape(pack_meta.shape)
    for kind, ref in enumerate((mid_ref, cot_ref)):
        chosen = mm(pick, ref[...], TN).astype(BF16)
        for g in range(GROUPS):
            pack[g, kind] = chosen[g * gcap : (g + 1) * gcap]
    met(count)

    def z_copy(step, there):
        target = lax.rem(z + step, GROUPS)
        return send(
            pack.at[target], zbuf.at[there], zs_sem.at[0, step], zr_sem.at[0, step], {"sp": target * plane + p}
        )

    def z_meta(step, there):
        target = lax.rem(z + step, GROUPS)
        return send(
            pack_meta.at[target], meta_ref.at[there], zs_sem.at[1, step], zr_sem.at[1, step],
            {"sp": target * plane + p},
        )

    for step in (2, 1, 3):
        z_meta(step, z).start()
        z_copy(step, z).start()
    meta_ref[z] = pack_meta[z]

    def x_copy(kind, turn, source, step, there):
        target = lax.rem(p + step, plane)
        return send(
            wide.at[turn, kind, target], rows_ref.at[kind, core, source, there],
            xs_sem.at[kind, turn, step], xr_sem.at[kind, turn, step], {"sp": z * plane + target},
        )

    def own_copy(kind, turn, source):
        return pltpu.make_async_copy(
            wide.at[turn, kind, p], rows_ref.at[kind, core, source, p], l_sem.at[kind, turn]
        )

    def expand(turn, source, mid, cot):
        table = meta_ref[source][:, : plane * cap]
        chosen = (table > 0).astype(F32).astype(BF16)
        ones = jnp.ones((gcap, 128), BF16)
        t3 = split3(table)
        column = (mm(t3[0], ones, TN) + (mm(t3[1], ones, TN) + mm(t3[2], ones, TN)))[:, :1]
        width = mid.shape[1]
        chunk = 512
        for n in range(0, width, chunk):
            cols = slice(n, n + chunk)
            wide[turn, 0, :, :, cols] = (
                mm(chosen, mid[:, cols], TN).reshape(plane, cap, chunk).astype(BF16)
            )
            wide[turn, 1, :, :, cols] = (
                (column * mm(chosen, cot[:, cols], TN)).reshape(plane, cap, chunk).astype(BF16)
            )
        for kind in range(2):
            loop(1, plane, lambda step: x_copy(kind, turn, source, step, p).start())
            own_copy(kind, turn, source).start()

    expand(0, z, pack.at[z, 0], pack.at[z, 1])

    length = q_ref.shape[0]
    heads = q_ref.shape[1] // DK
    mid_row = length // 2 - 1
    low = tri(length, True)
    low_b = low.astype(F32).astype(BF16)
    l3 = split3(ld_ref[...])
    rl = mm(low_b, l3[0]) + (mm(low_b, l3[1]) + mm(low_b, l3[2]))
    rl_ref[...] = rl
    dec_mine[...] = jnp.exp(rl[length - 1 :])
    def d_copy(step, there):
        target = lax.rem(mine + step, count)
        return send(dec_mine, decs_ref.at[there], ds.at[step], dr.at[step], {"sp": target})

    loop(1, count, lambda step: d_copy(step, mine).start())
    decs_ref[mine] = dec_mine[...]
    for h in range(heads):
        rl_h, mid, last, qs, kf = head_parts(rl, q_ref, k_ref, h, mid_row)
        value = v_ref[:, h * DV : (h + 1) * DV]
        to_end = split2(kf * jnp.exp(last - rl_h))
        total = mm2r(value, to_end, TN)
        total_ref[:, h * DK : (h + 1) * DK] = total
        scatter_pieces(piece, total, h)
    scan = Scan(piece, got, ready, inc_ref, decs_ref, s1, r1, s2, r2, False)
    scan.start()
    for h in range(heads):
        rl_h, mid, last, qs, kf = head_parts(rl, q_ref, k_ref, h, mid_row)
        up = split2(qs * jnp.exp(rl_h - mid))
        down = split2(kf * jnp.exp(mid - rl_h))
        score_ref[h] = jnp.where(low, mm3(up, down, NT), 0.0)

    for turn in range(1, GROUPS):
        step = (2, 1, 3)[turn - 1]
        source = lax.rem(z + GROUPS - step, GROUPS)
        z_meta(step, source).wait_recv()
        z_copy(step, source).wait_recv()
        expand(turn, source, zbuf.at[source, 0], zbuf.at[source, 1])

    loop(1, count, lambda step: d_copy(step, lax.rem(mine + count - step, count)).wait_recv())
    scan.middle()

    def forward(kind, turn, source, side):
        return send(
            rows_ref.at[kind, side, source], rows_ref.at[kind, side, source],
            fs_sem.at[kind, turn], fr_sem.at[kind, turn], {"tp": 1 - core},
        )

    for turn in range(GROUPS):
        source = lax.rem(z + GROUPS - (0, 2, 1, 3)[turn], GROUPS)
        for kind in range(2):
            own_copy(kind, turn, source).wait()
            loop(
                1, plane,
                lambda step: x_copy(kind, turn, source, step, lax.rem(p + plane - step, plane)).wait_recv(),
            )
            forward(kind, turn, source, core).start()

    scan.finish()
    for h in range(heads):
        rl_h, mid, last, qs, kf = head_parts(rl, q_ref, k_ref, h, mid_row)
        value = v_ref[:, h * DV : (h + 1) * DV]
        decayed = split2(qs * jnp.exp(rl_h))
        state = inc_ref[:, :, h * DK : (h + 1) * DK].reshape(DV, DK)
        raw = mm2l(split2(score_ref[h]), value) + mm2l(decayed, state, NT)
        inverse = lax.rsqrt(jnp.mean(raw * raw, axis=1, keepdims=True) + epsilon)
        out = raw * inverse
        normed_ref[:, h * DV : (h + 1) * DV] = out
        normed_rows_ref[:, h * DV : (h + 1) * DV] = out.astype(BF16)
        inv_ref[:, h * 128 : (h + 1) * 128] = jnp.broadcast_to(inverse, (length, 128))

    for turn in range(GROUPS):
        source = lax.rem(z + GROUPS - (0, 2, 1, 3)[turn], GROUPS)
        for kind in range(2):
            forward(kind, turn, source, core).wait_send()
            forward(kind, turn, source, 1 - core).wait_recv()
            loop(1, plane, lambda step: x_copy(kind, turn, source, step, p).wait_send())
    for step in (2, 1, 3):
        z_meta(step, z).wait_send()
        z_copy(step, z).wait_send()
    loop(1, count, lambda step: d_copy(step, mine).wait_send())
    scan.settle()


def front(mid, cot, experts, weights, q, k, v, ld):
    count = lax.axis_size("sp")
    plane = count // GROUPS
    rows, width = mid.shape
    cap = 4 * rows // count
    gcap = plane * cap // 2
    length, keys = q.shape
    heads = keys // DK
    dma = pltpu.SemaphoreType.DMA
    shape = jax.ShapeDtypeStruct
    vrows = DV // count
    outs = [
        shape((2, 2, GROUPS, plane, cap, width), BF16),
        shape((GROUPS, gcap, 128), F32),
        shape((rows, GROUPS * gcap), BF16),
        shape((count, 1, keys), F32),
        shape((count, vrows, keys), BF16),
        shape((length, heads * DV), F32),
        shape((length, heads * DV), BF16),
        shape((length, heads * 128), F32),
        shape((length, keys), F32),
        shape((heads, length, length), F32),
        shape((DV, keys), F32),
    ]
    return pl.pallas_call(
        front_kernel,
        out_shape=outs,
        in_specs=[pl.BlockSpec(memory_space=VMEM)] * 8,
        out_specs=[pl.BlockSpec(memory_space=VMEM)] * len(outs),
        scratch_shapes=[
            VMEM((GROUPS, 2, gcap, width), BF16),
            VMEM((GROUPS, gcap, 128), F32),
            VMEM((GROUPS, 2, gcap, width), BF16),
            VMEM((GROUPS, 2, plane, cap, width), BF16),
            VMEM((count, vrows, keys), BF16),
            VMEM((count, vrows, keys), BF16),
            VMEM((count, vrows, keys), BF16),
            VMEM((1, keys), F32),
            dma((2, GROUPS)), dma((2, GROUPS)),
            dma((2, GROUPS, plane)), dma((2, GROUPS, plane)),
            dma((2, GROUPS)), dma((2, GROUPS)), dma((2, GROUPS)),
            dma((count,)), dma((count,)), dma((count,)), dma((count,)), dma((count,)), dma((count,)),
        ],
        compiler_params=pltpu.CompilerParams(collective_id=0, has_side_effects=True),
        name="front",
    )(mid, cot, experts, weights, q, k, v, ld)


def expert_kernel(
    rows_ref, gate_ref, up_ref, down_ref, meta_ref, pick_ref, cot_ref, normed_ref,
    gate_out, up_out, down_out, token_ref, near_ref,
    hidden, back_gate, back_up, part, taken, whole, landed, comb, home,
    ns, nr, ps, pr, es, er, cs, cr,
):
    count, plane, mine, z, p, core = place()
    gcap = comb.shape[1]
    cap = whole.shape[2]
    half = part.shape[1] * part.shape[2]
    group_rows = part.shape[2]
    width = rows_ref.shape[2]
    hide = gate_ref.shape[1]
    greet_near()
    met(plane + GROUPS - 1)

    def n_copy(step, there):
        target = lax.rem(p + step, plane)
        return send(normed_ref, near_ref.at[there], ns.at[step], nr.at[step], {"sp": z * plane + target})

    loop(1, plane, lambda step: n_copy(step, p).start())
    near_ref[p] = normed_ref[...]

    def p_copy(g):
        return send(part.at[1 - core, g], taken.at[g], ps.at[g], pr.at[g], {"tp": 1 - core})

    def compute(side):
        base = pl.multiple_of(side * half, half)
        span = pl.ds(base, half)

        def inner(n):
            cols = pl.ds(pl.multiple_of(n * 256, 256), 256)
            pre_gate = mm(rows_ref[0, span, :], gate_ref[:, cols])
            pre_up = mm(rows_ref[0, span, :], up_ref[:, cols])
            back = mm(rows_ref[1, span, :], down_ref[cols, :], NT)
            sig = jax.nn.sigmoid(pre_gate)
            swish = pre_gate * sig
            hidden[span, cols] = (swish * pre_up).astype(BF16)
            back_up[span, cols] = (back * swish).astype(BF16)
            back_gate[span, cols] = (back * pre_up * (sig * (1.0 + pre_gate * (1.0 - sig)))).astype(BF16)

        loop(0, hide // 256, inner)

        def outer(n):
            cols = pl.ds(pl.multiple_of(n * 256, 256), 256)
            value = mm(back_gate[span, :], gate_ref[cols, :], NT) + mm(back_up[span, :], up_ref[cols, :], NT)
            part[side, :, :, cols] = value.astype(BF16).reshape(GROUPS, group_rows, 256)

        loop(0, width // 256, outer)

    compute(1 - core)
    order = [lax.rem(z + step, GROUPS) for step in (2, 1, 3, 0)]
    for g in order:
        p_copy(g).start()
    compute(core)

    def e_copy(turn, g, step, there):
        target = lax.rem(p + step, plane)
        return send(
            whole.at[turn, target], landed.at[turn, there], es.at[turn, step], er.at[turn, step],
            {"sp": z * plane + target},
        )

    for turn, g in enumerate(order):
        p_copy(g).wait_recv()
        value = part[core, g].astype(F32) + taken[g].astype(F32)
        whole[turn] = value.astype(BF16).reshape(plane, cap, width)
        loop(1, plane, lambda step: e_copy(turn, g, step, p).start())
        landed[turn, p] = whole[turn, p]

    def gates(n):
        cols = pl.ds(pl.multiple_of(n * 256, 256), 256)
        gate_out[cols, :] = mm(rows_ref[0, :, cols], back_gate[...], TN).astype(BF16)
        up_out[cols, :] = mm(rows_ref[0, :, cols], back_up[...], TN).astype(BF16)

    loop(0, width // 256, gates)

    def c_copy(turn, g, there):
        return send(comb.at[turn], home.at[there], cs.at[turn], cr.at[turn], {"sp": g * plane + p})

    for turn, g in enumerate(order):
        loop(1, plane, lambda step: e_copy(turn, g, step, lax.rem(p + plane - step, plane)).wait_recv())
        table = meta_ref[g][:, : plane * cap]
        chosen = (table > 0).astype(F32).astype(BF16)
        value = mm(chosen, landed[turn].reshape(plane * cap, width)).astype(BF16)
        if turn < GROUPS - 1:
            comb[turn] = value
            c_copy(turn, g, z).start()
        else:
            home[z] = value

    def downs(n):
        cols = pl.ds(pl.multiple_of(n * 256, 256), 256)
        down_out[cols, :] = mm(hidden[:, cols], rows_ref[1], TN).astype(BF16)

    loop(0, hide // 256, downs)

    for turn in range(GROUPS - 1):
        step = (2, 1, 3)[turn]
        c_copy(turn, z, lax.rem(z + GROUPS - step, GROUPS)).wait_recv()
    token_ref[...] = (
        cot_ref[...].astype(F32) + mm(pick_ref[...], home[...].reshape(GROUPS * gcap, width))
    ).astype(BF16)

    for turn, g in enumerate(order):
        p_copy(g).wait_send()
        loop(1, plane, lambda step: e_copy(turn, g, step, p).wait_send())
        if turn < GROUPS - 1:
            c_copy(turn, g, z).wait_send()
    loop(1, plane, lambda step: n_copy(step, p).wait_send())
    loop(1, plane, lambda step: n_copy(step, lax.rem(p + plane - step, plane)).wait_recv())


def experts_stage(rows, gate, up, down, meta, pick, cot, normed_rows):
    count = lax.axis_size("sp")
    plane = count // GROUPS
    cap = rows.shape[4]
    width = rows.shape[5]
    rows = rows.reshape(2, -1, width)
    total = rows.shape[1]
    hide = gate.shape[1]
    gcap = meta.shape[1]
    dma = pltpu.SemaphoreType.DMA
    shape = jax.ShapeDtypeStruct
    outs = [
        shape(gate.shape, BF16),
        shape(up.shape, BF16),
        shape(down.shape, BF16),
        shape(cot.shape, BF16),
        shape((plane,) + normed_rows.shape, BF16),
    ]
    return pl.pallas_call(
        expert_kernel,
        out_shape=outs,
        in_specs=[pl.BlockSpec(memory_space=VMEM)] * 8,
        out_specs=[pl.BlockSpec(memory_space=VMEM)] * len(outs),
        scratch_shapes=[
            VMEM((total, hide), BF16),
            VMEM((total, hide), BF16),
            VMEM((total, hide), BF16),
            VMEM((2, GROUPS, plane * cap, width), BF16),
            VMEM((GROUPS, plane * cap, width), BF16),
            VMEM((GROUPS, plane, cap, width), BF16),
            VMEM((GROUPS, plane, cap, width), BF16),
            VMEM((GROUPS - 1, gcap, width), BF16),
            VMEM((GROUPS, gcap, width), BF16),
            dma((plane,)), dma((plane,)),
            dma((GROUPS,)), dma((GROUPS,)),
            dma((GROUPS, plane)), dma((GROUPS, plane)),
            dma((GROUPS,)), dma((GROUPS,)),
        ],
        compiler_params=pltpu.CompilerParams(collective_id=1, has_side_effects=True),
        name="experts",
    )(rows, gate, up, down, meta, pick, cot, normed_rows)


def back_kernel(
    token_ref, weight_ref, near_ref, normed_ref, inv_ref, rl_ref, score_ref, inc_ref, decs_ref, total_ref,
    q_ref, k_ref, v_ref,
    out_ref, dq_ref, dk_ref, dv_ref, da_ref,
    both, cut, tok, own, give, take, raw, piece, got, ready, fut, run,
    ts, tr, ks, kr, os, orr, s1, r1, s2, r2,
):
    count, plane, mine, z, p, core = place()
    rows, width = token_ref.shape
    share = width // count
    length = q_ref.shape[0]
    heads = q_ref.shape[1] // DK
    mid_row = length // 2 - 1
    greet_all()
    met(count)

    def t_copy(side):
        return send(token_ref, both.at[side], ts, tr, {"tp": 1 - core})

    t_copy(core).start()
    both[core] = token_ref[...]
    t_copy(1 - core).wait_recv()

    for other in range(plane):
        for g in range(GROUPS):
            start = (g * plane + other) * share
            for side in range(2):
                cut[other, side * rows : (side + 1) * rows, g * share : (g + 1) * share] = both[
                    side, :, start : start + share
                ]

    def k_copy(step, there):
        target = lax.rem(p + step, plane)
        return send(cut.at[target], tok.at[there], ks.at[step], kr.at[step], {"sp": z * plane + target})

    loop(1, plane, lambda step: k_copy(step, p).start())
    tok[p] = cut[p]

    rl = rl_ref[...]
    for h in range(heads):
        cols = slice(h * DV, (h + 1) * DV)
        back = mm(both[...].reshape(length, width), weight_ref[:, cols])
        normed = normed_ref[:, cols]
        mean = jnp.mean(back * normed, axis=1, keepdims=True)
        inverse = inv_ref[:, h * 128 : h * 128 + 1]
        value = inverse * (back - normed * mean)
        raw[:, cols] = value
        rl_h, mid, last, qs, kf = head_parts(rl, q_ref, k_ref, h, mid_row)
        scatter_pieces(piece, mm3(split2(value), split2(qs * jnp.exp(rl_h)), TN), h)
    scan = Scan(piece, got, ready, fut, decs_ref, s1, r1, s2, r2, True)
    scan.start()

    def o_copy(step, there):
        target = lax.rem(z + step, GROUPS)
        return send(give.at[target], take.at[there], os.at[step], orr.at[step], {"sp": target * plane + p})

    loop(1, plane, lambda step: k_copy(step, lax.rem(p + plane - step, plane)).wait_recv())
    near = near_ref[...].reshape(plane * length, near_ref.shape[2])
    for g in range(GROUPS):
        value = mm(tok[:, :, g * share : (g + 1) * share].reshape(plane * length, share), near, TN)
        own[g] = value
        give[g] = value.astype(BF16)

    low = tri(length, True)
    scan.middle()
    for step in (2, 1, 3):
        o_copy(step, z).start()

    def parts(h):
        rl_h, mid, last, qs, kf = head_parts(rl, q_ref, k_ref, h, mid_row)
        cols = slice(h * DK, (h + 1) * DK)
        wide = slice(h * DV, (h + 1) * DV)
        return (rl_h, mid, last, qs, kf, cols, wide, v_ref[:, wide], split2(raw[:, wide]))

    for h in range(heads):
        rl_h, mid, last, qs, kf, cols, wide, value, back = parts(h)
        dots = split2(jnp.where(low, mm2l(back, value, NT), 0.0))
        up_scale, down_scale = jnp.exp(rl_h - mid), jnp.exp(mid - rl_h)
        state = inc_ref[:, :, cols].reshape(DV, DK)
        dq = up_scale * mm3(dots, split2(kf * down_scale)) + jnp.exp(rl_h) * mm2l(back, state)
        dq_ref[:, cols] = (dq * DK ** (-0.5)).astype(BF16)
        dk = down_scale * mm3(dots, split2(qs * up_scale), TN)
        run[0, :, cols] = dk
        run[1, :, cols] = qs * dq
        own_value = mm3(split2(score_ref[h]), back, TN)
        raw[:, wide] = own_value

    scan.finish()
    high_b = tri(length, False).astype(F32).astype(BF16)
    for h in range(heads):
        rl_h, mid, last, qs, kf = head_parts(rl, q_ref, k_ref, h, mid_row)
        cols = slice(h * DK, (h + 1) * DK)
        wide = slice(h * DV, (h + 1) * DV)
        value = v_ref[:, wide]
        future = fut[:, :, cols].reshape(DV, DK)
        to_end = jnp.exp(last - rl_h)
        dk = run[0, :, cols] + to_end * mm(value, future)
        dk_ref[:, cols] = dk.astype(BF16)
        dv_ref[:, wide] = (raw[:, wide] + mm2l(split2(kf * to_end), future, NT)).astype(BF16)
        change = run[1, :, cols] - kf * dk
        c3 = split3(change)
        later = mm(high_b, c3[0]) + (mm(high_b, c3[1]) + mm(high_b, c3[2]))
        state = inc_ref[:, :, cols].reshape(DV, DK).astype(F32)
        end = jnp.exp(last) * state + total_ref[:, cols]
        cross = jnp.sum(end * future.astype(F32), axis=0, keepdims=True)
        da_ref[:, cols] = later + cross

    for step in (2, 1, 3):
        o_copy(step, lax.rem(z + GROUPS - step, GROUPS)).wait_recv()
    sides = [lax.rem(z + step, GROUPS) for step in (1, 2, 3)]
    out_ref[...] = (own[z] + take[sides[0]].astype(F32)) + (
        take[sides[1]].astype(F32) + take[sides[2]].astype(F32)
    )

    t_copy(core).wait_send()
    loop(1, plane, lambda step: k_copy(step, p).wait_send())
    for step in (2, 1, 3):
        o_copy(step, z).wait_send()
    scan.settle()


def back_stage(token, weight, near, normed, inv, rl, score, inc, decs, total, q, k, v):
    count = lax.axis_size("sp")
    plane = count // GROUPS
    rows, width = token.shape
    share = width // count
    length, keys = q.shape
    values = v.shape[1]
    vrows = DV // count
    dma = pltpu.SemaphoreType.DMA
    shape = jax.ShapeDtypeStruct
    outs = [
        shape((share, values), F32),
        shape(q.shape, BF16),
        shape(k.shape, BF16),
        shape(v.shape, BF16),
        shape(q.shape, F32),
    ]
    return pl.pallas_call(
        back_kernel,
        out_shape=outs,
        in_specs=[pl.BlockSpec(memory_space=VMEM)] * 13,
        out_specs=[pl.BlockSpec(memory_space=VMEM)] * len(outs),
        scratch_shapes=[
            VMEM((2, rows, width), BF16),
            VMEM((plane, length, GROUPS * share), BF16),
            VMEM((plane, length, GROUPS * share), BF16),
            VMEM((GROUPS, share, values), F32),
            VMEM((GROUPS, share, values), BF16),
            VMEM((GROUPS, share, values), BF16),
            VMEM((length, values), F32),
            VMEM((count, vrows, keys), BF16),
            VMEM((count, vrows, keys), BF16),
            VMEM((count, vrows, keys), BF16),
            VMEM((count, vrows, keys), BF16),
            VMEM((2, length, keys), F32),
            dma, dma,
            dma((plane,)), dma((plane,)),
            dma((GROUPS,)), dma((GROUPS,)),
            dma((count,)), dma((count,)), dma((count,)), dma((count,)),
        ],
        compiler_params=pltpu.CompilerParams(collective_id=2, has_side_effects=True),
        name="back",
    )(token, weight, near, normed, inv, rl, score, inc, decs, total, q, k, v)


def body(
    mid_rows,
    cotangent,
    route_experts,
    route_weights,
    gate_weight,
    up_weight,
    down_weight,
    out_weight,
    queries,
    key_rows,
    value_rows,
    log_decay,
):
    rows, meta, pick, decs, inc, normed, normed_rows, inv, rl, score, total = front(
        mid_rows, cotangent, route_experts, route_weights, queries, key_rows, value_rows, log_decay
    )
    gate_grad, up_grad, down_grad, token, near = experts_stage(
        rows, gate_weight[0], up_weight[0], down_weight[0], meta, pick, cotangent, normed_rows
    )
    out_grad, dq, dk, dv, da = back_stage(
        token, out_weight, near, normed, inv, rl, score, inc, decs, total, queries, key_rows, value_rows
    )
    return (gate_grad[None], up_grad[None], down_grad[None], out_grad, dq, dk, dv, da)


def solution(mesh):
    in_specs = (
        P(("sp", "tp"), None),
        P(("sp", "tp"), None),
        P(("sp", "tp"), None),
        P(("sp", "tp"), None),
        P("sp", None, "tp"),
        P("sp", None, "tp"),
        P("sp", "tp", None),
        P(None, "tp"),
        P("sp", "tp"),
        P("sp", "tp"),
        P("sp", "tp"),
        P("sp", "tp"),
    )
    out_specs = (
        P("sp", None, "tp"),
        P("sp", None, "tp"),
        P("sp", "tp", None),
        P("sp", "tp"),
        P("sp", "tp"),
        P("sp", "tp"),
        P("sp", "tp"),
        P("sp", "tp"),
    )
    return jax.shard_map(body, mesh=mesh, in_specs=in_specs, out_specs=out_specs, check_vma=False)
```

```python
import functools
import types

import jax
import jax.numpy as jnp
from jax import lax
from jax.experimental import pallas as pl
from jax.experimental.pallas import tpu as pltpu
from jax.sharding import PartitionSpec as P

DK = 128
DV = 256
BLOCK = 64
GROUPS = 4

MESH = pl.DeviceIdType.MESH
F32 = jnp.float32
BF16 = jnp.bfloat16
epsilon = 1e-06
NN = (((1,), (0,)), ((), ()))
NT = (((1,), (1,)), ((), ()))
TN = (((0,), (0,)), ((), ()))
VMEM = pltpu.VMEM


def mm(a, b, dims=NN):
    return lax.dot_general(a, b, dims, preferred_element_type=F32)


def split2(x):
    high = x.astype(BF16)
    return (high, (x - high.astype(F32)).astype(BF16))


def split3(x):
    high, _ = split2(x)
    rest = x - high.astype(F32)
    return (high,) + split2(rest)


def mm3(a, b, dims=NN):
    return mm(a[0], b[0], dims) + (mm(a[0], b[1], dims) + mm(a[1], b[0], dims))


def mm2l(a, b, dims=NN):
    return mm(a[0], b, dims) + mm(a[1], b, dims)


def mm2r(a, b, dims=NN):
    return mm(a, b[0], dims) + mm(a, b[1], dims)


def place():
    count = lax.axis_size("sp")
    plane = count // GROUPS
    mine = lax.axis_index("sp")
    return (count, plane, mine, mine // plane, lax.rem(mine, plane), lax.axis_index("tp"))


def loop(low, high, act):
    def turn(step, carry):
        act(step)
        return carry

    lax.fori_loop(low, high, turn, 0)


def signal(where):
    pl.semaphore_signal(
        pltpu.get_barrier_semaphore(), inc=1, device_id=where, device_id_type=MESH
    )


def greet_all():
    count, plane, mine, z, p, core = place()
    loop(1, count, lambda step: signal({"sp": lax.rem(mine + step, count)}))
    signal({"tp": 1 - core})


def greet_near():
    count, plane, mine, z, p, core = place()
    loop(1, plane, lambda step: signal({"sp": z * plane + lax.rem(p + step, plane)}))
    loop(1, GROUPS, lambda step: signal({"sp": lax.rem(z + step, GROUPS) * plane + p}))
    signal({"tp": 1 - core})


def met(total):
    pl.semaphore_wait(pltpu.get_barrier_semaphore(), total)


def send(source, target, send_sem, recv_sem, where):
    return pltpu.make_async_remote_copy(
        src_ref=source,
        dst_ref=target,
        send_sem=send_sem,
        recv_sem=recv_sem,
        device_id=where,
        device_id_type=MESH,
    )


def tri(size, lower, strict=False):
    row = lax.broadcasted_iota(jnp.int32, (size, size), 0)
    col = lax.broadcasted_iota(jnp.int32, (size, size), 1)
    if lower:
        return row > col if strict else row >= col
    return row <= col


def head_parts(rl, q, k, h, mid_row):
    cols = slice(h * DK, (h + 1) * DK)
    rl_h = rl[:, cols]
    mid = rl_h[mid_row : mid_row + 1]
    last = rl_h[rl_h.shape[0] - 1 :]
    qs = q[:, cols].astype(F32) * DK ** (-0.5)
    kf = k[:, cols].astype(F32)
    return (rl_h, mid, last, qs, kf)


def scatter_pieces(target, value, h):
    count, rows = target.shape[0], target.shape[1]
    cols = slice(h * DK, (h + 1) * DK)
    for j in range(count):
        target[j, :, cols] = value[j * rows : (j + 1) * rows].astype(target.dtype)


class Scan:
    def __init__(self, total, got, ready, out, decs, s1, r1, s2, r2, backward):
        self.refs = (total, got, ready, out, decs)
        self.sems = (s1, r1, s2, r2)
        self.backward = backward

    def first(self, step, there):
        total, got, ready, out, decs = self.refs
        count, plane, mine, z, p, core = place()
        ahead = lax.rem(mine + step, count)
        return send(
            total.at[ahead], got.at[there], self.sems[0].at[step], self.sems[1].at[step], {"sp": ahead}
        )

    def second(self, step, there):
        total, got, ready, out, decs = self.refs
        count, plane, mine, z, p, core = place()
        ahead = lax.rem(mine + step, count)
        return send(
            ready.at[ahead], out.at[there], self.sems[2].at[step], self.sems[3].at[step], {"sp": ahead}
        )

    def start(self):
        total, got, ready, out, decs = self.refs
        count, plane, mine, z, p, core = place()
        loop(1, count, lambda step: self.first(step, mine).start())
        got[mine] = total[mine]

    def middle(self):
        total, got, ready, out, decs = self.refs
        count, plane, mine, z, p, core = place()
        loop(1, count, lambda step: self.first(step, lax.rem(mine + count - step, count)).wait_recv())

        def turn(position, carry):
            index = count - 1 - position if self.backward else position
            ready[index] = carry.astype(ready.dtype)
            return carry * decs[index] + got[index].astype(F32)

        lax.fori_loop(0, count, turn, jnp.zeros(got.shape[1:], F32))
        loop(1, count, lambda step: self.second(step, mine).start())
        out[mine] = ready[mine]

    def finish(self):
        count, plane, mine, z, p, core = place()
        loop(1, count, lambda step: self.second(step, lax.rem(mine + count - step, count)).wait_recv())

    def settle(self):
        count, plane, mine, z, p, core = place()

        def act(step):
            self.first(step, mine).wait_send()
            self.second(step, mine).wait_send()

        loop(1, count, act)


STEPS = (0, 2, 1, 3)
FIRST = ("ex", "wt", "mid", "cot", "ld", "q", "k", "v")
LATER = ("gate", "up", "down", "weight")


def column(row, eye):
    return jnp.sum(jnp.where(eye, row, 0.0), axis=1, keepdims=True)


def whole_kernel(names, *refs):
    r = types.SimpleNamespace(**dict(zip(names, refs)))
    count, plane, mine, z, p, core = place()
    greet_all()
    tokens, width = r.mid.shape
    cap = r.rows.shape[4]
    gcap = plane * cap // 2
    slots = plane * cap
    hide = r.gate.shape[1]
    length = r.q.shape[0]
    heads = r.q.shape[1] // DK
    mid_row = length // 2 - 1
    share = width // count
    low = tri(length, True)
    source_of = [lax.rem(z + GROUPS - step, GROUPS) for step in STEPS]

    loads = {
        name: pltpu.make_async_copy(getattr(r, name + "_in"), getattr(r, name), r.load_sem.at[n])
        for n, name in enumerate(FIRST + LATER)
    }
    for name in FIRST:
        loads[name].start()
    for name in FIRST[:4]:
        loads[name].wait()

    lane = lax.broadcasted_iota(jnp.int32, (tokens, 128), 1)
    lane_f = lane.astype(F32)
    eye = lax.broadcasted_iota(jnp.int32, (tokens, tokens), 0) == lax.broadcasted_iota(
        jnp.int32, (tokens, tokens), 1
    )
    chosen_experts = r.ex[...].astype(F32)
    e0, e1 = column(chosen_experts[0:1], eye), column(chosen_experts[1:2], eye)
    w0, w1 = column(r.wt[0:1, :], eye), column(r.wt[1:2, :], eye)
    hit0, hit1 = (e0 == lane_f), (e1 == lane_f)
    earlier = tri(tokens, True, True).astype(F32).astype(BF16)
    first_lane = lane_f * plane
    member = ((e0 >= first_lane) & (e0 < first_lane + plane)).astype(F32)
    named = (hit0.astype(F32) + hit1.astype(F32)).astype(BF16)
    before = mm(earlier, named)
    ahead_count = mm(earlier, member.astype(BF16))
    rank_group = jnp.sum(member * ahead_count, axis=1, keepdims=True)
    group = jnp.sum(member * lane_f, axis=1, keepdims=True)
    pick = (group * gcap + rank_group == lane_f).astype(F32).astype(BF16)
    r.pick[...] = pick
    for kind, ref in enumerate((r.mid, r.cot)):
        chosen = mm(pick, ref[...], TN).astype(BF16)
        for g in range(GROUPS):
            r.pack[g, kind] = chosen[g * gcap : (g + 1) * gcap]
    rank0 = jnp.sum(jnp.where(hit0, before, 0.0), axis=1, keepdims=True)
    rank1 = jnp.sum(jnp.where(hit1, before, 0.0), axis=1, keepdims=True)
    slot0 = (e0 - group * plane) * cap + rank0
    slot1 = (e1 - group * plane) * cap + rank1
    weights = jnp.where(slot0 == lane_f, w0, 0.0) + jnp.where(slot1 == lane_f, w1, 0.0)
    w3 = split3(weights)
    packed_meta = mm(pick, w3[0], TN) + (mm(pick, w3[1], TN) + mm(pick, w3[2], TN))
    r.pack_meta[...] = packed_meta.reshape(r.pack_meta.shape)
    met(count)

    def z_copy(step, there):
        target = lax.rem(z + step, GROUPS)
        return send(
            r.pack.at[target], r.zbuf.at[there], r.zs.at[0, step], r.zr.at[0, step],
            {"sp": target * plane + p},
        )

    def z_meta(step, there):
        target = lax.rem(z + step, GROUPS)
        return send(
            r.pack_meta.at[target], r.meta.at[there], r.zs.at[1, step], r.zr.at[1, step],
            {"sp": target * plane + p},
        )

    for step in STEPS[1:]:
        z_meta(step, z).start()
        z_copy(step, z).start()
    r.meta[z] = r.pack_meta[z]
    for name in LATER:
        loads[name].start()

    def x_copy(kind, turn, step, there):
        target = lax.rem(p + step, plane)
        return send(
            r.wide.at[turn, kind, target], r.rows.at[kind, turn, core, there],
            r.xs.at[kind, turn, step], r.xr.at[kind, turn, step], {"sp": z * plane + target},
        )

    def own_copy(kind, turn):
        return pltpu.make_async_copy(
            r.wide.at[turn, kind, p], r.rows.at[kind, turn, core, p], r.own_sem.at[kind, turn]
        )

    def expand(turn, mid, cot):
        table = r.meta[source_of[turn]][:, :slots]
        chosen = (table > 0).astype(F32).astype(BF16)
        ones = jnp.ones((gcap, 128), BF16)
        t3 = split3(table)
        scale = (mm(t3[0], ones, TN) + (mm(t3[1], ones, TN) + mm(t3[2], ones, TN)))[:, :1]
        chunk = 512
        for kind, ref in enumerate((mid, cot)):
            for n in range(0, width, chunk):
                cols = slice(n, n + chunk)
                value = mm(chosen, ref[:, cols], TN)
                if kind:
                    value = scale * value
                r.wide[turn, kind, :, :, cols] = value.reshape(plane, cap, chunk).astype(BF16)
            loop(1, plane, lambda step: x_copy(kind, turn, step, p).start())
            own_copy(kind, turn).start()

    def receive(turn):
        step, source = STEPS[turn], source_of[turn]
        z_meta(step, source).wait_recv()
        z_copy(step, source).wait_recv()
        expand(turn, r.zbuf.at[source, 0], r.zbuf.at[source, 1])

    def forward(kind, turn, side):
        return send(
            r.rows.at[kind, turn, side], r.rows.at[kind, turn, side],
            r.fs.at[kind, turn], r.fr.at[kind, turn], {"tp": 1 - core},
        )

    def arrive(turn):
        for kind in range(2):
            own_copy(kind, turn).wait()
            loop(
                1, plane,
                lambda step: x_copy(kind, turn, step, lax.rem(p + plane - step, plane)).wait_recv(),
            )
            forward(kind, turn, core).start()

    def p_copy(turn):
        return send(r.part.at[turn, 1 - core], r.taken.at[turn], r.ps.at[turn], r.pr.at[turn], {"tp": 1 - core})

    def compute(turn):
        for kind in range(2):
            forward(kind, turn, 1 - core).wait_recv()
        many = 2 * slots

        def inner(n):
            cols = pl.ds(pl.multiple_of(n * 256, 256), 256)
            rows = r.rows[0, turn].reshape(many, width)
            pre_gate = mm(rows, r.gate[:, cols])
            pre_up = mm(rows, r.up[:, cols])
            back = mm(r.rows[1, turn].reshape(many, width), r.down[cols, :], NT)
            sig = jax.nn.sigmoid(pre_gate)
            swish = pre_gate * sig
            r.hidden[turn, :, cols] = (swish * pre_up).astype(BF16)
            r.back_up[turn, :, cols] = (back * swish).astype(BF16)
            r.back_gate[turn, :, cols] = (back * pre_up * (sig * (1.0 + pre_gate * (1.0 - sig)))).astype(BF16)

        loop(0, hide // 256, inner)

        def outer(n):
            cols = pl.ds(pl.multiple_of(n * 512, 512), 512)
            value = mm(r.back_gate[turn], r.gate[cols, :], NT) + mm(r.back_up[turn], r.up[cols, :], NT)
            r.part[turn, :, :, cols] = value.astype(BF16).reshape(2, slots, 512)

        loop(0, width // 512, outer)
        p_copy(turn).start()

    def e_copy(turn, step, there):
        target = lax.rem(p + step, plane)
        return send(
            r.result.at[turn, target], r.landed.at[turn, there], r.es.at[turn, step], r.er.at[turn, step],
            {"sp": z * plane + target},
        )

    def give_back(turn):
        p_copy(turn).wait_recv()
        value = r.part[turn, core].astype(F32) + r.taken[turn].astype(F32)
        r.result[turn] = value.astype(BF16).reshape(plane, cap, width)
        loop(1, plane, lambda step: e_copy(turn, step, p).start())
        r.landed[turn, p] = r.result[turn, p]

    def c_copy(turn, there):
        return send(
            r.comb.at[turn], r.home.at[there], r.cs.at[turn], r.cr.at[turn],
            {"sp": source_of[turn] * plane + p},
        )

    def combine(turn):
        loop(1, plane, lambda step: e_copy(turn, step, lax.rem(p + plane - step, plane)).wait_recv())
        table = r.meta[source_of[turn]][:, :slots]
        chosen = (table > 0).astype(F32).astype(BF16)
        value = mm(chosen, r.landed[turn].reshape(slots, width)).astype(BF16)
        if turn:
            r.comb[turn] = value
            c_copy(turn, z).start()
        else:
            r.home[z] = value

    expand(0, r.pack.at[z, 0], r.pack.at[z, 1])

    for name in FIRST[4:]:
        loads[name].wait()
    low_b = low.astype(F32).astype(BF16)
    l3 = split3(r.ld[...])
    r.rl[...] = mm(low_b, l3[0]) + (mm(low_b, l3[1]) + mm(low_b, l3[2]))
    r.dec_mine[...] = jnp.exp(r.rl[length - 1 :, :])

    def d_copy(step, there):
        target = lax.rem(mine + step, count)
        return send(r.dec_mine, r.decs.at[there], r.ds.at[step], r.dr.at[step], {"sp": target})

    loop(1, count, lambda step: d_copy(step, mine).start())
    r.decs[mine] = r.dec_mine[...]

    def head(h):
        return head_parts(r.rl[...], r.q, r.k, h, mid_row)

    for h in range(heads):
        rl_h, mid, last, qs, kf = head(h)
        value = r.v[:, h * DV : (h + 1) * DV]
        to_end = split2(kf * jnp.exp(last - rl_h))
        total = mm2r(value, to_end, TN)
        r.total[:, h * DK : (h + 1) * DK] = total
        scatter_pieces(r.piece, total, h)
    scan = Scan(r.piece, r.got, r.ready, r.inc, r.decs, r.s1, r.r1, r.s2, r.r2, False)
    scan.start()

    arrive(0)
    receive(1)
    for name in LATER[:3]:
        loads[name].wait()
    compute(0)
    receive(2)
    arrive(1)
    give_back(0)
    compute(1)
    receive(3)
    arrive(2)
    give_back(1)
    combine(0)
    compute(2)
    loop(1, count, lambda step: d_copy(step, lax.rem(mine + count - step, count)).wait_recv())
    scan.middle()
    arrive(3)
    give_back(2)
    combine(1)
    compute(3)
    combine(2)
    give_back(3)

    scan.finish()

    def n_copy(step, there):
        target = lax.rem(p + step, plane)
        return send(r.normed_rows, r.near.at[there], r.ns.at[step], r.nr.at[step], {"sp": z * plane + target})

    for h in range(heads):
        rl_h, mid, last, qs, kf = head(h)
        wide = slice(h * DV, (h + 1) * DV)
        up = split2(qs * jnp.exp(rl_h - mid))
        down = split2(kf * jnp.exp(mid - rl_h))
        score = jnp.where(low, mm3(up, down, NT), 0.0)
        r.score[h] = score
        decayed = split2(qs * jnp.exp(rl_h))
        state = r.inc[:, :, h * DK : (h + 1) * DK].reshape(DV, DK)
        raw = mm2l(split2(score), r.v[:, wide]) + mm2l(decayed, state, NT)
        inverse = lax.rsqrt(jnp.mean(raw * raw, axis=1, keepdims=True) + epsilon)
        out = raw * inverse
        r.normed[:, wide] = out
        r.normed_rows[:, wide] = out.astype(BF16)
        r.inv[:, h * 128 : (h + 1) * 128] = jnp.broadcast_to(inverse, (length, 128))
    r.near[p] = r.normed_rows[...]
    loop(1, plane, lambda step: n_copy(step, p).start())

    combine(3)
    all_rows = GROUPS * 2 * slots

    def gates(n):
        cols = pl.ds(pl.multiple_of(n * 256, 256), 256)
        rows = r.rows[0, :, :, :, :, cols].reshape(all_rows, 256)
        r.gate_out[cols, :] = mm(rows, r.back_gate[...].reshape(all_rows, hide), TN).astype(BF16)
        r.up_out[cols, :] = mm(rows, r.back_up[...].reshape(all_rows, hide), TN).astype(BF16)

    loop(0, width // 256, gates)

    for turn in range(1, GROUPS):
        c_copy(turn, lax.rem(z + STEPS[turn], GROUPS)).wait_recv()
    token = (
        r.cot[...].astype(F32) + mm(r.pick[...], r.home[...].reshape(GROUPS * gcap, width))
    ).astype(BF16)
    r.token[...] = token
    r.both[core] = token

    def t_copy(side):
        return send(r.token, r.both.at[side], r.ts, r.tr, {"tp": 1 - core})

    t_copy(core).start()
    t_copy(1 - core).wait_recv()

    for other in range(plane):
        for g in range(GROUPS):
            start = (g * plane + other) * share
            for side in range(2):
                r.cut[other, side * tokens : (side + 1) * tokens, g * share : (g + 1) * share] = r.both[
                    side, :, start : start + share
                ]

    def k_copy(step, there):
        target = lax.rem(p + step, plane)
        return send(r.cut.at[target], r.tok.at[there], r.ks.at[step], r.kr.at[step], {"sp": z * plane + target})

    loop(1, plane, lambda step: k_copy(step, p).start())
    r.tok[p] = r.cut[p]

    loads["weight"].wait()
    for h in range(heads):
        wide = slice(h * DV, (h + 1) * DV)
        back = mm(r.both[...].reshape(length, width), r.weight[:, wide])
        normed = r.normed[:, wide]
        mean = jnp.mean(back * normed, axis=1, keepdims=True)
        inverse = r.inv[:, h * 128 : h * 128 + 1]
        value = inverse * (back - normed * mean)
        r.raw[:, wide] = value
        rl_h, mid, last, qs, kf = head(h)
        scatter_pieces(r.piece2, mm3(split2(value), split2(qs * jnp.exp(rl_h)), TN), h)
    scan2 = Scan(r.piece2, r.got2, r.ready2, r.fut, r.decs, r.s3, r.r3, r.s4, r.r4, True)
    scan2.start()

    def o_copy(step, there):
        target = lax.rem(z + step, GROUPS)
        return send(
            r.give.at[target], r.take.at[there], r.os.at[step], r.orr.at[step], {"sp": target * plane + p}
        )

    for h in range(heads):
        rl_h, mid, last, qs, kf = head(h)
        cols = slice(h * DK, (h + 1) * DK)
        wide = slice(h * DV, (h + 1) * DV)
        back = split2(r.raw[:, wide])
        dots = split2(jnp.where(low, mm2l(back, r.v[:, wide], NT), 0.0))
        up_scale, down_scale = jnp.exp(rl_h - mid), jnp.exp(mid - rl_h)
        state = r.inc[:, :, cols].reshape(DV, DK)
        dq = up_scale * mm3(dots, split2(kf * down_scale)) + jnp.exp(rl_h) * mm2l(back, state)
        r.dq[:, cols] = (dq * DK ** (-0.5)).astype(BF16)
        r.run[0, :, cols] = down_scale * mm3(dots, split2(qs * up_scale), TN)
        r.run[1, :, cols] = qs * dq
        r.raw[:, wide] = mm3(split2(r.score[h]), back, TN)

    loop(1, plane, lambda step: k_copy(step, lax.rem(p + plane - step, plane)).wait_recv())
    loop(1, plane, lambda step: n_copy(step, lax.rem(p + plane - step, plane)).wait_recv())
    near = r.near[...].reshape(plane * length, r.near.shape[2])
    for g in range(GROUPS):
        value = mm(r.tok[:, :, g * share : (g + 1) * share].reshape(plane * length, share), near, TN)
        r.own[g] = value
        r.give[g] = value.astype(BF16)
    o_copy(1, z).start()
    scan2.middle()
    o_copy(2, z).start()
    o_copy(3, z).start()

    def downs(n):
        cols = pl.ds(pl.multiple_of(n * 256, 256), 256)
        hidden = r.hidden[:, :, cols].reshape(all_rows, 256)
        r.down_out[cols, :] = mm(hidden, r.rows[1].reshape(all_rows, width), TN).astype(BF16)

    loop(0, hide // 256, downs)

    scan2.finish()
    high_b = tri(length, False).astype(F32).astype(BF16)
    for h in range(heads):
        rl_h, mid, last, qs, kf = head(h)
        cols = slice(h * DK, (h + 1) * DK)
        wide = slice(h * DV, (h + 1) * DV)
        future = r.fut[:, :, cols].reshape(DV, DK)
        to_end = jnp.exp(last - rl_h)
        dk = r.run[0, :, cols] + to_end * mm(r.v[:, wide], future)
        r.dk[:, cols] = dk.astype(BF16)
        r.dv[:, wide] = (r.raw[:, wide] + mm2l(split2(kf * to_end), future, NT)).astype(BF16)
        change = split3(r.run[1, :, cols] - kf * dk)
        later = mm(high_b, change[0]) + (mm(high_b, change[1]) + mm(high_b, change[2]))
        state = r.inc[:, :, cols].reshape(DV, DK).astype(F32)
        end = jnp.exp(last) * state + r.total[:, cols]
        r.da[:, cols] = later + jnp.sum(end * future.astype(F32), axis=0, keepdims=True)

    for step in STEPS[1:]:
        o_copy(step, lax.rem(z + GROUPS - step, GROUPS)).wait_recv()
    sides = [lax.rem(z + step, GROUPS) for step in (1, 2, 3)]
    r.out[...] = (r.own[z] + r.take[sides[0]].astype(F32)) + (
        r.take[sides[1]].astype(F32) + r.take[sides[2]].astype(F32)
    )

    for step in STEPS[1:]:
        z_meta(step, z).wait_send()
        z_copy(step, z).wait_send()
        o_copy(step, z).wait_send()
    for turn in range(GROUPS):
        for kind in range(2):
            loop(1, plane, lambda step: x_copy(kind, turn, step, p).wait_send())
            forward(kind, turn, core).wait_send()
        p_copy(turn).wait_send()
        loop(1, plane, lambda step: e_copy(turn, step, p).wait_send())
        if turn:
            c_copy(turn, z).wait_send()
    loop(1, count, lambda step: d_copy(step, mine).wait_send())

    def near_sends(step):
        n_copy(step, p).wait_send()
        k_copy(step, p).wait_send()

    loop(1, plane, near_sends)
    t_copy(core).wait_send()
    scan.settle()
    scan2.settle()


def whole(mid, cot, experts, weights, gate, up, down, weight, q, k, v, ld):
    count = lax.axis_size("sp")
    plane = count // GROUPS
    tokens, width = mid.shape
    cap = 4 * tokens // count
    slots = plane * cap
    gcap = slots // 2
    length, keys = q.shape
    heads = keys // DK
    values = v.shape[1]
    hide = gate.shape[1]
    share = width // count
    vrows = DV // count
    shape = jax.ShapeDtypeStruct
    dma = pltpu.SemaphoreType.DMA
    given = dict(
        mid=mid, cot=cot, ex=experts, wt=weights, q=q, k=k, v=v, ld=ld,
        gate=gate, up=up, down=down, weight=weight,
    )
    ins = {name + "_in": value for name, value in given.items()}
    outs = dict(
        gate_out=shape(gate.shape, BF16), up_out=shape(up.shape, BF16), down_out=shape(down.shape, BF16),
        out=shape((share, values), F32), dq=shape(q.shape, BF16), dk=shape(k.shape, BF16),
        dv=shape(v.shape, BF16), da=shape(q.shape, F32),
    )
    pieces = VMEM((count, vrows, keys), BF16)
    g3 = dma((2, GROUPS))
    scratch = {name: VMEM(value.shape, value.dtype) for name, value in given.items()}
    scratch |= dict(
        pick=VMEM((tokens, GROUPS * gcap), BF16),
        pack=VMEM((GROUPS, 2, gcap, width), BF16),
        pack_meta=VMEM((GROUPS, gcap, 128), F32),
        meta=VMEM((GROUPS, gcap, 128), F32),
        zbuf=VMEM((GROUPS, 2, gcap, width), BF16),
        wide=VMEM((GROUPS, 2, plane, cap, width), BF16),
        rows=VMEM((2, GROUPS, 2, plane, cap, width), BF16),
        hidden=VMEM((GROUPS, 2 * slots, hide), BF16),
        back_gate=VMEM((GROUPS, 2 * slots, hide), BF16),
        back_up=VMEM((GROUPS, 2 * slots, hide), BF16),
        part=VMEM((GROUPS, 2, slots, width), BF16),
        taken=VMEM((GROUPS, slots, width), BF16),
        result=VMEM((GROUPS, plane, cap, width), BF16),
        landed=VMEM((GROUPS, plane, cap, width), BF16),
        comb=VMEM((GROUPS, gcap, width), BF16),
        home=VMEM((GROUPS, gcap, width), BF16),
        rl=VMEM((length, keys), F32), dec_mine=VMEM((1, keys), F32), decs=VMEM((count, 1, keys), F32),
        total=VMEM((DV, keys), F32), score=VMEM((heads, length, length), F32),
        normed=VMEM((length, values), F32), normed_rows=VMEM((length, values), BF16),
        inv=VMEM((length, heads * 128), F32), near=VMEM((plane, length, values), BF16),
        piece=pieces, got=pieces, ready=pieces, inc=pieces,
        piece2=pieces, got2=pieces, ready2=pieces, fut=pieces,
        token=VMEM((tokens, width), BF16), both=VMEM((2, tokens, width), BF16),
        cut=VMEM((plane, length, GROUPS * share), BF16), tok=VMEM((plane, length, GROUPS * share), BF16),
        raw=VMEM((length, values), F32), run=VMEM((2, length, keys), F32),
        own=VMEM((GROUPS, share, values), F32), give=VMEM((GROUPS, share, values), BF16),
        take=VMEM((GROUPS, share, values), BF16),
        load_sem=dma((12,)), zs=g3, zr=g3, own_sem=g3, fs=g3, fr=g3,
        xs=dma((2, GROUPS, plane)), xr=dma((2, GROUPS, plane)),
        ps=dma((GROUPS,)), pr=dma((GROUPS,)), es=dma((GROUPS, plane)), er=dma((GROUPS, plane)),
        cs=dma((GROUPS,)), cr=dma((GROUPS,)), ds=dma((count,)), dr=dma((count,)),
        ns=dma((plane,)), nr=dma((plane,)), ks=dma((plane,)), kr=dma((plane,)), ts=dma, tr=dma,
        os=dma((GROUPS,)), orr=dma((GROUPS,)),
        s1=dma((count,)), r1=dma((count,)), s2=dma((count,)), r2=dma((count,)),
        s3=dma((count,)), r3=dma((count,)), s4=dma((count,)), r4=dma((count,)),
    )
    vmem = pl.BlockSpec(memory_space=VMEM)
    return pl.pallas_call(
        functools.partial(whole_kernel, tuple(ins) + tuple(outs) + tuple(scratch)),
        out_shape=list(outs.values()),
        in_specs=[pl.BlockSpec(memory_space=pltpu.HBM)] * len(ins),
        out_specs=[vmem] * len(outs),
        scratch_shapes=list(scratch.values()),
        compiler_params=pltpu.CompilerParams(
            collective_id=0, has_side_effects=True, vmem_limit_bytes=LIMIT
        ),
        name="whole",
    )(*[pltpu.with_memory_space_constraint(x, pltpu.HBM) for x in ins.values()])


LIMIT = 44 * 2**20


def emit_kernel(number, *refs):
    copies = [
        pltpu.make_async_copy(refs[n], refs[number + n], refs[2 * number].at[n]) for n in range(number)
    ]
    for copy in copies:
        copy.start()
    for copy in copies:
        copy.wait()


def emit(values):
    number = len(values)
    return pl.pallas_call(
        functools.partial(emit_kernel, number),
        out_shape=[jax.ShapeDtypeStruct(x.shape, x.dtype) for x in values],
        in_specs=[pl.BlockSpec(memory_space=VMEM)] * number,
        out_specs=[pl.BlockSpec(memory_space=pl.ANY)] * number,
        scratch_shapes=[pltpu.SemaphoreType.DMA((number,))],
        compiler_params=pltpu.CompilerParams(vmem_limit_bytes=12 * 2**20),
        name="emit",
    )(*values)


def body(
    mid_rows,
    cotangent,
    route_experts,
    route_weights,
    gate_weight,
    up_weight,
    down_weight,
    out_weight,
    queries,
    key_rows,
    value_rows,
    log_decay,
):
    results = whole(
        mid_rows, cotangent, route_experts.T, route_weights.T, gate_weight[0], up_weight[0], down_weight[0],
        out_weight, queries, key_rows, value_rows, log_decay,
    )
    gate_grad, up_grad, down_grad, out_grad, dq, dk, dv, da = emit(results)
    return (gate_grad[None], up_grad[None], down_grad[None], out_grad, dq, dk, dv, da)


def solution(mesh):
    in_specs = (
        P(("sp", "tp"), None),
        P(("sp", "tp"), None),
        P(("sp", "tp"), None),
        P(("sp", "tp"), None),
        P("sp", None, "tp"),
        P("sp", None, "tp"),
        P("sp", "tp", None),
        P(None, "tp"),
        P("sp", "tp"),
        P("sp", "tp"),
        P("sp", "tp"),
        P("sp", "tp"),
    )
    out_specs = (
        P("sp", None, "tp"),
        P("sp", None, "tp"),
        P("sp", "tp", None),
        P("sp", "tp"),
        P("sp", "tp"),
        P("sp", "tp"),
        P("sp", "tp"),
        P("sp", "tp"),
    )
    return jax.shard_map(body, mesh=mesh, in_specs=in_specs, out_specs=out_specs, check_vma=False)
```

```python
import functools
import types

import jax
import jax.numpy as jnp
from jax import lax
from jax.experimental import pallas as pl
from jax.experimental.pallas import tpu as pltpu
from jax.sharding import PartitionSpec as P

DK = 128
DV = 256
BLOCK = 64
GROUPS = 4

MESH = pl.DeviceIdType.MESH
F32 = jnp.float32
BF16 = jnp.bfloat16
epsilon = 1e-06
NN = (((1,), (0,)), ((), ()))
NT = (((1,), (1,)), ((), ()))
TN = (((0,), (0,)), ((), ()))
VMEM = pltpu.VMEM


def mm(a, b, dims=NN):
    return lax.dot_general(a, b, dims, preferred_element_type=F32)


def split2(x):
    high = x.astype(BF16)
    return (high, (x - high.astype(F32)).astype(BF16))


def split3(x):
    high, _ = split2(x)
    rest = x - high.astype(F32)
    return (high,) + split2(rest)


def mm3(a, b, dims=NN):
    return mm(a[0], b[0], dims) + (mm(a[0], b[1], dims) + mm(a[1], b[0], dims))


def mm2l(a, b, dims=NN):
    return mm(a[0], b, dims) + mm(a[1], b, dims)


def mm2r(a, b, dims=NN):
    return mm(a, b[0], dims) + mm(a, b[1], dims)


def place():
    count = lax.axis_size("sp")
    plane = count // GROUPS
    mine = lax.axis_index("sp")
    return (count, plane, mine, mine // plane, lax.rem(mine, plane), lax.axis_index("tp"))


def loop(low, high, act):
    def turn(step, carry):
        act(step)
        return carry

    lax.fori_loop(low, high, turn, 0)


def signal(where):
    pl.semaphore_signal(
        pltpu.get_barrier_semaphore(), inc=1, device_id=where, device_id_type=MESH
    )


def greet_all():
    count, plane, mine, z, p, core = place()
    loop(1, count, lambda step: signal({"sp": lax.rem(mine + step, count)}))
    signal({"tp": 1 - core})


def met(total):
    pl.semaphore_wait(pltpu.get_barrier_semaphore(), total)


def send(source, target, send_sem, recv_sem, where):
    return pltpu.make_async_remote_copy(
        src_ref=source,
        dst_ref=target,
        send_sem=send_sem,
        recv_sem=recv_sem,
        device_id=where,
        device_id_type=MESH,
    )


def tri(size, lower, strict=False):
    row = lax.broadcasted_iota(jnp.int32, (size, size), 0)
    col = lax.broadcasted_iota(jnp.int32, (size, size), 1)
    if lower:
        return row > col if strict else row >= col
    return row <= col


def head_parts(rl, q, k, h, mid_row):
    cols = slice(h * DK, (h + 1) * DK)
    rl_h = rl[:, cols]
    mid = rl_h[mid_row : mid_row + 1]
    last = rl_h[rl_h.shape[0] - 1 :]
    qs = q[:, cols].astype(F32) * DK ** (-0.5)
    kf = k[:, cols].astype(F32)
    return (rl_h, mid, last, qs, kf)


def scatter_pieces(target, value, h):
    count, rows = target.shape[0], target.shape[1]
    cols = slice(h * DK, (h + 1) * DK)
    for j in range(count):
        target[j, :, cols] = value[j * rows : (j + 1) * rows].astype(target.dtype)


class Scan:
    def __init__(self, total, got, lift, zgot, ready, out, decs, zdecs, s1, r1, s2, r2, s3, r3, backward):
        self.refs = (total, got, lift, zgot, ready, out, decs)
        self.sems = (s1, r1, s2, r2, s3, r3)
        self.backward = backward
        self.zdecs = zdecs

    def flat(self, last, step, there):
        total, got, lift, zgot, ready, out, decs = self.refs
        count, plane, mine, z, p, core = place()
        target = lax.rem(p + step, plane)
        source, place_there = (ready, out) if last else (total, got)
        sems = self.sems[4:] if last else self.sems[:2]
        return send(
            source.at[target], place_there.at[there], sems[0].at[step], sems[1].at[step],
            {"sp": z * plane + target},
        )

    def rise(self, step):
        total, got, lift, zgot, ready, out, decs = self.refs
        count, plane, mine, z, p, core = place()
        target = z - step if self.backward else z + step
        ok = target >= 0 if self.backward else target < GROUPS
        return (ok, send(lift, zgot.at[z], self.sems[2].at[step], self.sems[3].at[step], {"sp": target * plane + p}))

    def fall(self, step):
        total, got, lift, zgot, ready, out, decs = self.refs
        count, plane, mine, z, p, core = place()
        source = z + step if self.backward else z - step
        ok = source < GROUPS if self.backward else source >= 0
        return (ok, send(lift, zgot.at[source], self.sems[2].at[step], self.sems[3].at[step], {"sp": mine}))

    def spot(self, position, size):
        return size - 1 - position if self.backward else position

    def start(self):
        total, got, lift, zgot, ready, out, decs = self.refs
        count, plane, mine, z, p, core = place()
        loop(1, plane, lambda step: self.flat(False, step, p).start())
        got[p] = total[p]

    def up(self):
        total, got, lift, zgot, ready, out, decs = self.refs
        count, plane, mine, z, p, core = place()
        loop(1, plane, lambda step: self.flat(False, step, lax.rem(p + plane - step, plane)).wait_recv())

        def turn(position, carry):
            index = self.spot(position, plane)
            return carry * decs[index] + got[index].astype(F32)

        lift[...] = lax.fori_loop(0, plane, turn, jnp.zeros(lift.shape, F32)).astype(lift.dtype)
        for step in range(1, GROUPS):
            ok, copy = self.rise(step)
            pl.when(ok)(copy.start)

    def down(self):
        total, got, lift, zgot, ready, out, decs = self.refs
        count, plane, mine, z, p, core = place()
        for step in range(1, GROUPS):
            ok, copy = self.fall(step)
            pl.when(ok)(copy.wait_recv)

        def over(position, carry):
            index = self.spot(position, GROUPS)
            return carry * self.zdecs[index] + zgot[index].astype(F32)

        carry = lax.fori_loop(
            0, GROUPS - 1 - z if self.backward else z, over, jnp.zeros(lift.shape, F32)
        )

        def turn(position, carry):
            index = self.spot(position, plane)
            ready[index] = carry.astype(ready.dtype)
            return carry * decs[index] + got[index].astype(F32)

        lax.fori_loop(0, plane, turn, carry)
        loop(1, plane, lambda step: self.flat(True, step, p).start())
        out[p] = ready[p]

    def finish(self):
        count, plane, mine, z, p, core = place()
        loop(1, plane, lambda step: self.flat(True, step, lax.rem(p + plane - step, plane)).wait_recv())

    def settle(self):
        count, plane, mine, z, p, core = place()

        def act(step):
            self.flat(False, step, p).wait_send()
            self.flat(True, step, p).wait_send()

        loop(1, plane, act)
        for step in range(1, GROUPS):
            ok, copy = self.rise(step)
            pl.when(ok)(copy.wait_send)


STEPS = (0, 2, 1, 3)
FIRST = ("ex", "wt", "mid", "cot", "ld", "q", "k", "v")
LATER = ("gate", "up", "down", "weight")


def column(row, eye):
    return jnp.sum(jnp.where(eye, row, 0.0), axis=1, keepdims=True)


def whole_kernel(names, *refs):
    r = types.SimpleNamespace(**dict(zip(names, refs)))
    count, plane, mine, z, p, core = place()
    greet_all()
    tokens, width = r.mid.shape
    cap = r.rows.shape[4]
    gcap = plane * cap // 2
    slots = plane * cap
    hide = r.gate.shape[1]
    length = r.q.shape[0]
    heads = r.q.shape[1] // DK
    mid_row = length // 2 - 1
    share = width // count
    low = tri(length, True)
    source_of = [lax.rem(z + GROUPS - step, GROUPS) for step in STEPS]

    loads = {
        name: pltpu.make_async_copy(getattr(r, name + "_in"), getattr(r, name), r.load_sem.at[n])
        for n, name in enumerate(FIRST + LATER)
    }
    for name in FIRST:
        loads[name].start()
    for name in FIRST[:4]:
        loads[name].wait()

    lane = lax.broadcasted_iota(jnp.int32, (tokens, 128), 1)
    lane_f = lane.astype(F32)
    eye = lax.broadcasted_iota(jnp.int32, (tokens, tokens), 0) == lax.broadcasted_iota(
        jnp.int32, (tokens, tokens), 1
    )
    chosen_experts = r.ex[...].astype(F32)
    e0, e1 = column(chosen_experts[0:1], eye), column(chosen_experts[1:2], eye)
    w0, w1 = column(r.wt[0:1, :], eye), column(r.wt[1:2, :], eye)
    hit0, hit1 = (e0 == lane_f), (e1 == lane_f)
    earlier = tri(tokens, True, True).astype(F32).astype(BF16)
    first_lane = lane_f * plane
    member = ((e0 >= first_lane) & (e0 < first_lane + plane)).astype(F32)
    named = (hit0.astype(F32) + hit1.astype(F32)).astype(BF16)
    before = mm(earlier, named)
    ahead_count = mm(earlier, member.astype(BF16))
    rank_group = jnp.sum(member * ahead_count, axis=1, keepdims=True)
    group = jnp.sum(member * lane_f, axis=1, keepdims=True)
    pick = (group * gcap + rank_group == lane_f).astype(F32).astype(BF16)
    r.pick[...] = pick
    for kind, ref in enumerate((r.mid, r.cot)):
        chosen = mm(pick, ref[...], TN).astype(BF16)
        for g in range(GROUPS):
            r.pack[g, kind] = chosen[g * gcap : (g + 1) * gcap]
    rank0 = jnp.sum(jnp.where(hit0, before, 0.0), axis=1, keepdims=True)
    rank1 = jnp.sum(jnp.where(hit1, before, 0.0), axis=1, keepdims=True)
    slot0 = (e0 - group * plane) * cap + rank0
    slot1 = (e1 - group * plane) * cap + rank1
    weights = jnp.where(slot0 == lane_f, w0, 0.0) + jnp.where(slot1 == lane_f, w1, 0.0)
    w3 = split3(weights)
    packed_meta = mm(pick, w3[0], TN) + (mm(pick, w3[1], TN) + mm(pick, w3[2], TN))
    r.pack_meta[...] = packed_meta.reshape(r.pack_meta.shape)
    met(count)

    def z_copy(kind, step, there):
        target = lax.rem(z + step, GROUPS)
        return send(
            r.pack.at[target, kind], r.zbuf.at[there, kind], r.zs.at[kind, step], r.zr.at[kind, step],
            {"sp": target * plane + p},
        )

    def z_meta(step, there):
        target = lax.rem(z + step, GROUPS)
        return send(
            r.pack_meta.at[target], r.meta.at[there], r.zs.at[2, step], r.zr.at[2, step],
            {"sp": target * plane + p},
        )

    for step in STEPS[1:]:
        z_meta(step, z).start()
        for kind in range(2):
            z_copy(kind, step, z).start()
    r.meta[z] = r.pack_meta[z]
    for name in LATER:
        loads[name].start()

    def x_copy(kind, turn, step, there):
        target = lax.rem(p + step, plane)
        return send(
            r.wide.at[turn, kind, target], r.rows.at[kind, turn, core, there],
            r.xs.at[kind, turn, step], r.xr.at[kind, turn, step], {"sp": z * plane + target},
        )

    def own_copy(kind, turn):
        return pltpu.make_async_copy(
            r.wide.at[turn, kind, p], r.rows.at[kind, turn, core, p], r.own_sem.at[kind, turn]
        )

    def expand(kind, turn, ref):
        table = r.meta[source_of[turn]][:, :slots]
        chosen = (table > 0).astype(F32).astype(BF16)
        if kind:
            ones = jnp.ones((gcap, 128), BF16)
            t3 = split3(table)
            scale = (mm(t3[0], ones, TN) + (mm(t3[1], ones, TN) + mm(t3[2], ones, TN)))[:, :1]
        chunk = 512
        for n in range(0, width, chunk):
            cols = slice(n, n + chunk)
            value = mm(chosen, ref[:, cols], TN)
            if kind:
                value = scale * value
            r.wide[turn, kind, :, :, cols] = value.reshape(plane, cap, chunk).astype(BF16)
        loop(1, plane, lambda step: x_copy(kind, turn, step, p).start())
        own_copy(kind, turn).start()

    def receive(turn):
        step, source = STEPS[turn], source_of[turn]
        z_meta(step, source).wait_recv()
        for kind in range(2):
            z_copy(kind, step, source).wait_recv()
            expand(kind, turn, r.zbuf.at[source, kind])

    def forward(kind, turn, side):
        return send(
            r.rows.at[kind, turn, side], r.rows.at[kind, turn, side],
            r.fs.at[kind, turn], r.fr.at[kind, turn], {"tp": 1 - core},
        )

    def arrive(turn):
        for kind in range(2):
            own_copy(kind, turn).wait()
            loop(
                1, plane,
                lambda step: x_copy(kind, turn, step, lax.rem(p + plane - step, plane)).wait_recv(),
            )
            forward(kind, turn, core).start()

    def p_copy(turn):
        return send(r.part.at[turn, 1 - core], r.taken.at[turn], r.ps.at[turn], r.pr.at[turn], {"tp": 1 - core})

    def compute(turn):
        for kind in range(2):
            forward(kind, turn, 1 - core).wait_recv()
        many = 2 * slots

        def inner(n):
            cols = pl.ds(pl.multiple_of(n * 256, 256), 256)
            rows = r.rows[0, turn].reshape(many, width)
            pre_gate = mm(rows, r.gate[:, cols])
            pre_up = mm(rows, r.up[:, cols])
            back = mm(r.rows[1, turn].reshape(many, width), r.down[cols, :], NT)
            sig = jax.nn.sigmoid(pre_gate)
            swish = pre_gate * sig
            r.hidden[turn, :, cols] = (swish * pre_up).astype(BF16)
            r.back_up[turn, :, cols] = (back * swish).astype(BF16)
            r.back_gate[turn, :, cols] = (back * pre_up * (sig * (1.0 + pre_gate * (1.0 - sig)))).astype(BF16)

        loop(0, hide // 256, inner)

        def outer(n):
            cols = pl.ds(pl.multiple_of(n * 512, 512), 512)
            value = mm(r.back_gate[turn], r.gate[cols, :], NT) + mm(r.back_up[turn], r.up[cols, :], NT)
            r.part[turn, :, :, cols] = value.astype(BF16).reshape(2, slots, 512)

        loop(0, width // 512, outer)
        p_copy(turn).start()

    def e_copy(turn, step, there):
        target = lax.rem(p + step, plane)
        return send(
            r.result.at[turn, target], r.landed.at[turn, there], r.es.at[turn, step], r.er.at[turn, step],
            {"sp": z * plane + target},
        )

    def give_back(turn):
        p_copy(turn).wait_recv()
        value = r.part[turn, core].astype(F32) + r.taken[turn].astype(F32)
        r.result[turn] = value.astype(BF16).reshape(plane, cap, width)
        loop(1, plane, lambda step: e_copy(turn, step, p).start())
        r.landed[turn, p] = r.result[turn, p]

    def c_copy(turn, there):
        return send(
            r.comb.at[turn], r.home.at[there], r.cs.at[turn], r.cr.at[turn],
            {"sp": source_of[turn] * plane + p},
        )

    def combine(turn):
        loop(1, plane, lambda step: e_copy(turn, step, lax.rem(p + plane - step, plane)).wait_recv())
        table = r.meta[source_of[turn]][:, :slots]
        chosen = (table > 0).astype(F32).astype(BF16)
        value = mm(chosen, r.landed[turn].reshape(slots, width)).astype(BF16)
        if turn:
            r.comb[turn] = value
            c_copy(turn, z).start()
        else:
            r.home[z] = value

    expand(0, 0, r.pack.at[z, 0])
    expand(1, 0, r.pack.at[z, 1])

    for name in FIRST[4:]:
        loads[name].wait()
    low_b = low.astype(F32).astype(BF16)
    l3 = split3(r.ld[...])
    r.rl[...] = mm(low_b, l3[0]) + (mm(low_b, l3[1]) + mm(low_b, l3[2]))
    r.dec_mine[...] = jnp.exp(r.rl[length - 1 :, :])

    def d_copy(step, there):
        target = lax.rem(p + step, plane)
        return send(r.dec_mine, r.decs.at[there], r.ds.at[step], r.dr.at[step], {"sp": z * plane + target})

    def w_copy(step, there):
        target = lax.rem(z + step, GROUPS)
        return send(r.dec_plane, r.zdecs.at[there], r.ws.at[step], r.wr.at[step], {"sp": target * plane + p})

    loop(1, plane, lambda step: d_copy(step, p).start())
    r.decs[p] = r.dec_mine[...]

    def head(h):
        return head_parts(r.rl[...], r.q, r.k, h, mid_row)

    for h in range(heads):
        rl_h, mid, last, qs, kf = head(h)
        value = r.v[:, h * DV : (h + 1) * DV]
        to_end = split2(kf * jnp.exp(last - rl_h))
        total = mm2r(value, to_end, TN)
        r.total[:, h * DK : (h + 1) * DK] = total
        scatter_pieces(r.piece, total, h)
    scan = Scan(r.piece, r.got, r.lift, r.zgot, r.ready, r.inc, r.decs, r.zdecs, r.s1, r.r1, r.s2, r.r2, r.s5, r.r5, False)
    scan.start()

    arrive(0)
    loop(1, plane, lambda step: d_copy(step, lax.rem(p + plane - step, plane)).wait_recv())
    r.dec_plane[...] = lax.fori_loop(0, plane, lambda n, x: x * r.decs[n], jnp.ones(r.dec_mine.shape, F32))
    loop(1, GROUPS, lambda step: w_copy(step, z).start())
    scan.up()
    for name in LATER[:3]:
        loads[name].wait()
    compute(0)
    receive(1)
    give_back(0)
    receive(2)
    arrive(1)
    receive(3)
    compute(1)
    arrive(2)
    combine(0)
    give_back(1)
    compute(2)
    loop(1, GROUPS, lambda step: w_copy(step, lax.rem(z + GROUPS - step, GROUPS)).wait_recv())
    scan.down()
    arrive(3)
    give_back(2)
    compute(3)
    combine(1)
    give_back(3)
    scan.finish()

    pair = z + 1 - 2 * lax.rem(z, 2)
    across = lax.rem(z + 2, GROUPS)

    far = lax.rem(pair + 2, GROUPS)

    def n_copy(step, there):
        target = lax.rem(p + step, plane)
        return send(r.normed_rows, r.near.at[there], r.ns.at[step], r.nr.at[step], {"sp": z * plane + target})

    for h in range(heads):
        rl_h, mid, last, qs, kf = head(h)
        wide = slice(h * DV, (h + 1) * DV)
        up = split2(qs * jnp.exp(rl_h - mid))
        down = split2(kf * jnp.exp(mid - rl_h))
        score = jnp.where(low, mm3(up, down, NT), 0.0)
        r.score[h] = score
        decayed = split2(qs * jnp.exp(rl_h))
        state = r.inc[:, :, h * DK : (h + 1) * DK].reshape(DV, DK)
        raw = mm2l(split2(score), r.v[:, wide]) + mm2l(decayed, state, NT)
        inverse = lax.rsqrt(jnp.mean(raw * raw, axis=1, keepdims=True) + epsilon)
        out = raw * inverse
        r.normed[:, wide] = out
        r.normed_rows[:, wide] = out.astype(BF16)
        r.inv[:, h * 128 : (h + 1) * 128] = jnp.broadcast_to(inverse, (length, 128))
    loop(1, plane, lambda step: n_copy(step, p).start())
    r.near[p] = r.normed_rows[...]
    combine(2)
    all_rows = GROUPS * 2 * slots

    def gates(n):
        cols = pl.ds(pl.multiple_of(n * 256, 256), 256)
        rows = r.rows[0, :, :, :, :, cols].reshape(all_rows, 256)
        r.gate_out[cols, :] = mm(rows, r.back_gate[...].reshape(all_rows, hide), TN).astype(BF16)
        r.up_out[cols, :] = mm(rows, r.back_up[...].reshape(all_rows, hide), TN).astype(BF16)

    loop(0, width // 256, gates)
    combine(3)

    def downs(n):
        cols = pl.ds(pl.multiple_of(n * 256, 256), 256)
        hidden = r.hidden[:, :, cols].reshape(all_rows, 256)
        r.down_out[cols, :] = mm(hidden, r.rows[1].reshape(all_rows, width), TN).astype(BF16)

    loop(0, hide // 256, downs)

    for turn in range(1, GROUPS):
        c_copy(turn, lax.rem(z + STEPS[turn], GROUPS)).wait_recv()
    token = (
        r.cot[...].astype(F32) + mm(r.pick[...], r.home[...].reshape(GROUPS * gcap, width))
    ).astype(BF16)
    r.token[...] = token
    for other in range(plane):
        for g in range(GROUPS):
            start = (g * plane + other) * share
            r.cut[other, g] = token[:, start : start + share]
    r.both[core] = token

    def t_copy(side):
        return send(r.token, r.both.at[side], r.ts, r.tr, {"tp": 1 - core})

    def k_copy(step, there):
        target = lax.rem(p + step, plane)
        return send(
            r.cut.at[target], r.tok.at[there, core], r.ks.at[step], r.kr.at[step], {"sp": z * plane + target}
        )

    def k_pass(step, side):
        there = lax.rem(p + plane - step, plane)
        return send(
            r.tok.at[there, side], r.tok.at[there, side], r.js.at[step], r.jr.at[step], {"tp": 1 - core}
        )

    t_copy(core).start()
    loop(1, plane, lambda step: k_copy(step, p).start())
    r.tok[p, core] = r.cut[p]
    k_pass(0, core).start()
    t_copy(1 - core).wait_recv()

    loads["weight"].wait()
    for h in range(heads):
        wide = slice(h * DV, (h + 1) * DV)
        back = mm(r.both[...].reshape(length, width), r.weight[:, wide])
        normed = r.normed[:, wide]
        mean = jnp.mean(back * normed, axis=1, keepdims=True)
        inverse = r.inv[:, h * 128 : h * 128 + 1]
        value = inverse * (back - normed * mean)
        r.raw[:, wide] = value
        rl_h, mid, last, qs, kf = head(h)
        scatter_pieces(r.piece2, mm3(split2(value), split2(qs * jnp.exp(rl_h)), TN), h)
    scan2 = Scan(r.piece2, r.got2, r.lift2, r.zgot2, r.ready2, r.fut, r.decs, r.zdecs, r.s3, r.r3, r.s4, r.r4, r.s6, r.r6, True)
    scan2.start()

    def o_copy(n):
        aim = across if n == 2 else pair
        return send(r.give.at[n], r.take.at[n], r.os.at[n], r.orr.at[n], {"sp": aim * plane + p})

    def terms(g):
        rows = plane * length
        return mm(r.tok[:, :, g].reshape(rows, share), r.near[...].reshape(rows, r.near.shape[2]), TN)

    for h in range(heads):
        rl_h, mid, last, qs, kf = head(h)
        cols = slice(h * DK, (h + 1) * DK)
        wide = slice(h * DV, (h + 1) * DV)
        back = split2(r.raw[:, wide])
        dots = split2(jnp.where(low, mm2l(back, r.v[:, wide], NT), 0.0))
        up_scale, down_scale = jnp.exp(rl_h - mid), jnp.exp(mid - rl_h)
        state = r.inc[:, :, cols].reshape(DV, DK)
        dq = up_scale * mm3(dots, split2(kf * down_scale)) + jnp.exp(rl_h) * mm2l(back, state)
        r.dq[:, cols] = (dq * DK ** (-0.5)).astype(BF16)
        r.run[0, :, cols] = down_scale * mm3(dots, split2(qs * up_scale), TN)
        r.run[1, :, cols] = qs * dq
        r.raw[:, wide] = mm3(split2(r.score[h]), back, TN)

    def k_arrive(step):
        k_copy(step, lax.rem(p + plane - step, plane)).wait_recv()
        k_pass(step, core).start()

    loop(1, plane, k_arrive)
    scan2.up()
    loop(0, plane, lambda step: k_pass(step, 1 - core).wait_recv())
    loop(1, plane, lambda step: n_copy(step, lax.rem(p + plane - step, plane)).wait_recv())
    for n, g in enumerate((far, pair)):
        r.give[n] = terms(g).astype(BF16)
        o_copy(n).start()
    r.own[1] = terms(across)
    r.own[0] = terms(z)
    o_copy(0).wait_recv()
    r.give[2] = (r.own[1] + r.take[0].astype(F32)).astype(BF16)
    o_copy(2).start()
    scan2.down()
    scan2.finish()
    high_b = tri(length, False).astype(F32).astype(BF16)
    for h in range(heads):
        rl_h, mid, last, qs, kf = head(h)
        cols = slice(h * DK, (h + 1) * DK)
        wide = slice(h * DV, (h + 1) * DV)
        future = r.fut[:, :, cols].reshape(DV, DK)
        to_end = jnp.exp(last - rl_h)
        dk = r.run[0, :, cols] + to_end * mm(r.v[:, wide], future)
        r.dk[:, cols] = dk.astype(BF16)
        r.dv[:, wide] = (r.raw[:, wide] + mm2l(split2(kf * to_end), future, NT)).astype(BF16)
        change = split3(r.run[1, :, cols] - kf * dk)
        later = mm(high_b, change[0]) + (mm(high_b, change[1]) + mm(high_b, change[2]))
        state = r.inc[:, :, cols].reshape(DV, DK).astype(F32)
        end = jnp.exp(last) * state + r.total[:, cols]
        r.da[:, cols] = later + jnp.sum(end * future.astype(F32), axis=0, keepdims=True)

    o_copy(1).wait_recv()
    o_copy(2).wait_recv()
    r.out[...] = r.own[0] + (r.take[1].astype(F32) + r.take[2].astype(F32))

    for n in range(3):
        o_copy(n).wait_send()
    for step in STEPS[1:]:
        z_meta(step, z).wait_send()
        for kind in range(2):
            z_copy(kind, step, z).wait_send()
    for turn in range(GROUPS):
        for kind in range(2):
            loop(1, plane, lambda step: x_copy(kind, turn, step, p).wait_send())
            forward(kind, turn, core).wait_send()
        p_copy(turn).wait_send()
        loop(1, plane, lambda step: e_copy(turn, step, p).wait_send())
        if turn:
            c_copy(turn, z).wait_send()
    loop(1, plane, lambda step: d_copy(step, p).wait_send())
    loop(1, GROUPS, lambda step: w_copy(step, z).wait_send())

    loop(1, plane, lambda step: n_copy(step, p).wait_send())
    loop(1, plane, lambda step: k_copy(step, p).wait_send())
    loop(0, plane, lambda step: k_pass(step, core).wait_send())
    t_copy(core).wait_send()
    scan.settle()
    scan2.settle()


def whole(mid, cot, experts, weights, gate, up, down, weight, q, k, v, ld):
    count = lax.axis_size("sp")
    plane = count // GROUPS
    tokens, width = mid.shape
    cap = 4 * tokens // count
    slots = plane * cap
    gcap = slots // 2
    length, keys = q.shape
    heads = keys // DK
    values = v.shape[1]
    hide = gate.shape[1]
    share = width // count
    shape = jax.ShapeDtypeStruct
    dma = pltpu.SemaphoreType.DMA
    given = dict(
        mid=mid, cot=cot, ex=experts, wt=weights, q=q, k=k, v=v, ld=ld,
        gate=gate, up=up, down=down, weight=weight,
    )
    ins = {name + "_in": value for name, value in given.items()}
    outs = dict(
        gate_out=shape(gate.shape, BF16), up_out=shape(up.shape, BF16), down_out=shape(down.shape, BF16),
        out=shape((share, values), F32), dq=shape(q.shape, BF16), dk=shape(k.shape, BF16),
        dv=shape(v.shape, BF16), da=shape(q.shape, F32),
    )
    pieces = VMEM((plane, DV // plane, keys), BF16)
    lifts = VMEM((DV // plane, keys), BF16)
    zgots = VMEM((GROUPS, DV // plane, keys), BF16)
    g3 = dma((2, GROUPS))
    scratch = {name: VMEM(value.shape, value.dtype) for name, value in given.items()}
    scratch |= dict(
        pick=VMEM((tokens, GROUPS * gcap), BF16),
        pack=VMEM((GROUPS, 2, gcap, width), BF16),
        pack_meta=VMEM((GROUPS, gcap, 128), F32),
        meta=VMEM((GROUPS, gcap, 128), F32),
        zbuf=VMEM((GROUPS, 2, gcap, width), BF16),
        wide=VMEM((GROUPS, 2, plane, cap, width), BF16),
        rows=VMEM((2, GROUPS, 2, plane, cap, width), BF16),
        hidden=VMEM((GROUPS, 2 * slots, hide), BF16),
        back_gate=VMEM((GROUPS, 2 * slots, hide), BF16),
        back_up=VMEM((GROUPS, 2 * slots, hide), BF16),
        part=VMEM((GROUPS, 2, slots, width), BF16),
        taken=VMEM((GROUPS, slots, width), BF16),
        result=VMEM((GROUPS, plane, cap, width), BF16),
        landed=VMEM((GROUPS, plane, cap, width), BF16),
        comb=VMEM((GROUPS, gcap, width), BF16),
        home=VMEM((GROUPS, gcap, width), BF16),
        rl=VMEM((length, keys), F32), dec_mine=VMEM((1, keys), F32), decs=VMEM((plane, 1, keys), F32), dec_plane=VMEM((1, keys), F32),
        zdecs=VMEM((GROUPS, 1, keys), F32),
        total=VMEM((DV, keys), F32), score=VMEM((heads, length, length), F32),
        normed=VMEM((length, values), F32), normed_rows=VMEM((length, values), BF16),
        inv=VMEM((length, heads * 128), F32), near=VMEM((plane, length, values), BF16),
        piece=pieces, got=pieces, ready=pieces, inc=pieces, lift=lifts, zgot=zgots, lift2=lifts, zgot2=zgots,
        piece2=pieces, got2=pieces, ready2=pieces, fut=pieces,
        token=VMEM((tokens, width), BF16), both=VMEM((2, tokens, width), BF16),
        cut=VMEM((plane, GROUPS, tokens, share), BF16), tok=VMEM((plane, 2, GROUPS, tokens, share), BF16),
        raw=VMEM((length, values), F32), run=VMEM((2, length, keys), F32),
        own=VMEM((2, share, values), F32), give=VMEM((3, share, values), BF16), take=VMEM((3, share, values), BF16),
        load_sem=dma((12,)), zs=dma((3, GROUPS)), zr=dma((3, GROUPS)), own_sem=g3, fs=g3, fr=g3,
        xs=dma((2, GROUPS, plane)), xr=dma((2, GROUPS, plane)),
        ps=dma((GROUPS,)), pr=dma((GROUPS,)), es=dma((GROUPS, plane)), er=dma((GROUPS, plane)),
        cs=dma((GROUPS,)), cr=dma((GROUPS,)), ds=dma((plane,)), dr=dma((plane,)),
        ws=dma((GROUPS,)), wr=dma((GROUPS,)),
        ns=dma((plane,)), nr=dma((plane,)), ks=dma((plane,)), kr=dma((plane,)), js=dma((plane,)), jr=dma((plane,)),
        ts=dma, tr=dma, os=dma((3,)), orr=dma((3,)),
        s1=dma((plane,)), r1=dma((plane,)), s2=dma((GROUPS,)), r2=dma((GROUPS,)), s5=dma((plane,)), r5=dma((plane,)),
        s3=dma((plane,)), r3=dma((plane,)), s4=dma((GROUPS,)), r4=dma((GROUPS,)), s6=dma((plane,)), r6=dma((plane,)),
    )
    vmem = pl.BlockSpec(memory_space=VMEM)
    return pl.pallas_call(
        functools.partial(whole_kernel, tuple(ins) + tuple(outs) + tuple(scratch)),
        out_shape=list(outs.values()),
        in_specs=[pl.BlockSpec(memory_space=pltpu.HBM)] * len(ins),
        out_specs=[vmem] * len(outs),
        scratch_shapes=list(scratch.values()),
        compiler_params=pltpu.CompilerParams(
            collective_id=0, has_side_effects=True, vmem_limit_bytes=LIMIT
        ),
        name="whole",
    )(*[pltpu.with_memory_space_constraint(x, pltpu.HBM) for x in ins.values()])


LIMIT = 44 * 2**20


def emit_kernel(number, *refs):
    copies = [
        pltpu.make_async_copy(refs[n], refs[number + n], refs[2 * number].at[n]) for n in range(number)
    ]
    for copy in copies:
        copy.start()
    for copy in copies:
        copy.wait()


def emit(values):
    number = len(values)
    return pl.pallas_call(
        functools.partial(emit_kernel, number),
        out_shape=[jax.ShapeDtypeStruct(x.shape, x.dtype) for x in values],
        in_specs=[pl.BlockSpec(memory_space=VMEM)] * number,
        out_specs=[pl.BlockSpec(memory_space=pl.ANY)] * number,
        scratch_shapes=[pltpu.SemaphoreType.DMA((number,))],
        compiler_params=pltpu.CompilerParams(vmem_limit_bytes=12 * 2**20),
        name="emit",
    )(*values)


def body(
    mid_rows,
    cotangent,
    route_experts,
    route_weights,
    gate_weight,
    up_weight,
    down_weight,
    out_weight,
    queries,
    key_rows,
    value_rows,
    log_decay,
):
    results = whole(
        mid_rows, cotangent, route_experts.T, route_weights.T, gate_weight[0], up_weight[0], down_weight[0],
        out_weight, queries, key_rows, value_rows, log_decay,
    )
    gate_grad, up_grad, down_grad, out_grad, dq, dk, dv, da = emit(results)
    return (gate_grad[None], up_grad[None], down_grad[None], out_grad, dq, dk, dv, da)


def solution(mesh):
    in_specs = (
        P(("sp", "tp"), None),
        P(("sp", "tp"), None),
        P(("sp", "tp"), None),
        P(("sp", "tp"), None),
        P("sp", None, "tp"),
        P("sp", None, "tp"),
        P("sp", "tp", None),
        P(None, "tp"),
        P("sp", "tp"),
        P("sp", "tp"),
        P("sp", "tp"),
        P("sp", "tp"),
    )
    out_specs = (
        P("sp", None, "tp"),
        P("sp", None, "tp"),
        P("sp", "tp", None),
        P("sp", "tp"),
        P("sp", "tp"),
        P("sp", "tp"),
        P("sp", "tp"),
        P("sp", "tp"),
    )
    return jax.shard_map(body, mesh=mesh, in_specs=in_specs, out_specs=out_specs, check_vma=False)
```

```python
import functools
import types

import jax
import jax.numpy as jnp
from jax import lax
from jax.experimental import pallas as pl
from jax.experimental.pallas import tpu as pltpu
from jax.sharding import PartitionSpec as P

DK = 128
DV = 256
BLOCK = 64
GROUPS = 4

MESH = pl.DeviceIdType.MESH
F32 = jnp.float32
BF16 = jnp.bfloat16
epsilon = 1e-06
NN = (((1,), (0,)), ((), ()))
NT = (((1,), (1,)), ((), ()))
TN = (((0,), (0,)), ((), ()))
VMEM = pltpu.VMEM


def mm(a, b, dims=NN):
    return lax.dot_general(a, b, dims, preferred_element_type=F32)


def split2(x):
    high = x.astype(BF16)
    return (high, (x - high.astype(F32)).astype(BF16))


def split3(x):
    high, _ = split2(x)
    rest = x - high.astype(F32)
    return (high,) + split2(rest)


def mm3(a, b, dims=NN):
    return mm(a[0], b[0], dims) + (mm(a[0], b[1], dims) + mm(a[1], b[0], dims))


def mm2l(a, b, dims=NN):
    return mm(a[0], b, dims) + mm(a[1], b, dims)


def mm2r(a, b, dims=NN):
    return mm(a, b[0], dims) + mm(a, b[1], dims)


def place():
    count = lax.axis_size("sp")
    plane = count // GROUPS
    mine = lax.axis_index("sp")
    return (count, plane, mine, mine // plane, lax.rem(mine, plane), lax.axis_index("tp"))


def loop(low, high, act):
    def turn(step, carry):
        act(step)
        return carry

    lax.fori_loop(low, high, turn, 0)


def signal(where):
    pl.semaphore_signal(
        pltpu.get_barrier_semaphore(), inc=1, device_id=where, device_id_type=MESH
    )


def greet_all():
    count, plane, mine, z, p, core = place()
    loop(1, count, lambda step: signal({"sp": lax.rem(mine + step, count)}))
    signal({"tp": 1 - core})


def met(total):
    pl.semaphore_wait(pltpu.get_barrier_semaphore(), total)


def send(source, target, send_sem, recv_sem, where):
    return pltpu.make_async_remote_copy(
        src_ref=source,
        dst_ref=target,
        send_sem=send_sem,
        recv_sem=recv_sem,
        device_id=where,
        device_id_type=MESH,
    )


def tri(size, lower, strict=False):
    row = lax.broadcasted_iota(jnp.int32, (size, size), 0)
    col = lax.broadcasted_iota(jnp.int32, (size, size), 1)
    if lower:
        return row > col if strict else row >= col
    return row <= col


def head_parts(rl, q, k, h, mid_row):
    cols = slice(h * DK, (h + 1) * DK)
    rl_h = rl[:, cols]
    mid = rl_h[mid_row : mid_row + 1]
    last = rl_h[rl_h.shape[0] - 1 :]
    qs = q[:, cols].astype(F32) * DK ** (-0.5)
    kf = k[:, cols].astype(F32)
    return (rl_h, mid, last, qs, kf)


def scatter_pieces(target, value, h):
    count, rows = target.shape[0], target.shape[1]
    cols = slice(h * DK, (h + 1) * DK)
    for j in range(count):
        target[j, :, cols] = value[j * rows : (j + 1) * rows].astype(target.dtype)


class Scan:
    def __init__(self, total, got, lift, zgot, ready, out, decs, zdecs, s1, r1, s2, r2, s3, r3, backward):
        self.refs = (total, got, lift, zgot, ready, out, decs)
        self.sems = (s1, r1, s2, r2, s3, r3)
        self.backward = backward
        self.zdecs = zdecs

    def flat(self, last, step, there):
        total, got, lift, zgot, ready, out, decs = self.refs
        count, plane, mine, z, p, core = place()
        target = lax.rem(p + step, plane)
        source, place_there = (ready, out) if last else (total, got)
        sems = self.sems[4:] if last else self.sems[:2]
        return send(
            source.at[target], place_there.at[there], sems[0].at[step], sems[1].at[step],
            {"sp": z * plane + target},
        )

    def rise(self, step):
        total, got, lift, zgot, ready, out, decs = self.refs
        count, plane, mine, z, p, core = place()
        target = z - step if self.backward else z + step
        ok = target >= 0 if self.backward else target < GROUPS
        return (ok, send(lift, zgot.at[z], self.sems[2].at[step], self.sems[3].at[step], {"sp": target * plane + p}))

    def fall(self, step):
        total, got, lift, zgot, ready, out, decs = self.refs
        count, plane, mine, z, p, core = place()
        source = z + step if self.backward else z - step
        ok = source < GROUPS if self.backward else source >= 0
        return (ok, send(lift, zgot.at[source], self.sems[2].at[step], self.sems[3].at[step], {"sp": mine}))

    def spot(self, position, size):
        return size - 1 - position if self.backward else position

    def start(self):
        total, got, lift, zgot, ready, out, decs = self.refs
        count, plane, mine, z, p, core = place()
        loop(1, plane, lambda step: self.flat(False, step, p).start())
        got[p] = total[p]

    def up(self):
        total, got, lift, zgot, ready, out, decs = self.refs
        count, plane, mine, z, p, core = place()
        loop(1, plane, lambda step: self.flat(False, step, lax.rem(p + plane - step, plane)).wait_recv())

        def turn(position, carry):
            index = self.spot(position, plane)
            return carry * decs[index] + got[index].astype(F32)

        lift[...] = lax.fori_loop(0, plane, turn, jnp.zeros(lift.shape, F32)).astype(lift.dtype)
        for step in range(1, GROUPS):
            ok, copy = self.rise(step)
            pl.when(ok)(copy.start)

    def down(self):
        total, got, lift, zgot, ready, out, decs = self.refs
        count, plane, mine, z, p, core = place()
        for step in range(1, GROUPS):
            ok, copy = self.fall(step)
            pl.when(ok)(copy.wait_recv)

        def over(position, carry):
            index = self.spot(position, GROUPS)
            return carry * self.zdecs[index] + zgot[index].astype(F32)

        carry = lax.fori_loop(
            0, GROUPS - 1 - z if self.backward else z, over, jnp.zeros(lift.shape, F32)
        )

        def turn(position, carry):
            index = self.spot(position, plane)
            ready[index] = carry.astype(ready.dtype)
            return carry * decs[index] + got[index].astype(F32)

        lax.fori_loop(0, plane, turn, carry)
        loop(1, plane, lambda step: self.flat(True, step, p).start())
        out[p] = ready[p]

    def finish(self):
        count, plane, mine, z, p, core = place()
        loop(1, plane, lambda step: self.flat(True, step, lax.rem(p + plane - step, plane)).wait_recv())

    def settle(self):
        count, plane, mine, z, p, core = place()

        def act(step):
            self.flat(False, step, p).wait_send()
            self.flat(True, step, p).wait_send()

        loop(1, plane, act)
        for step in range(1, GROUPS):
            ok, copy = self.rise(step)
            pl.when(ok)(copy.wait_send)


STEPS = (0, 3, 2, 1)
FIRST = ("ex", "wt", "mid", "cot", "ld", "q", "k", "v")
LATER = ("gate", "up", "down", "weight")


def column(row, eye):
    return jnp.sum(jnp.where(eye, row, 0.0), axis=1, keepdims=True)


def whole_kernel(names, *refs):
    r = types.SimpleNamespace(**dict(zip(names, refs)))
    count, plane, mine, z, p, core = place()
    greet_all()
    tokens, width = r.mid.shape
    cap = r.rows.shape[4]
    gcap = plane * cap // 2
    slots = plane * cap
    hide = r.gate.shape[1]
    length = r.q.shape[0]
    heads = r.q.shape[1] // DK
    mid_row = length // 2 - 1
    share = width // count
    low = tri(length, True)
    source_of = [lax.rem(z + GROUPS - step, GROUPS) for step in STEPS]

    loads = {
        name: pltpu.make_async_copy(getattr(r, name + "_in"), getattr(r, name), r.load_sem.at[n])
        for n, name in enumerate(FIRST + LATER)
    }
    for name in FIRST:
        loads[name].start()
    for name in FIRST[:4]:
        loads[name].wait()

    lane = lax.broadcasted_iota(jnp.int32, (tokens, 128), 1)
    lane_f = lane.astype(F32)
    eye = lax.broadcasted_iota(jnp.int32, (tokens, tokens), 0) == lax.broadcasted_iota(
        jnp.int32, (tokens, tokens), 1
    )
    chosen_experts = r.ex[...].astype(F32)
    e0, e1 = column(chosen_experts[0:1], eye), column(chosen_experts[1:2], eye)
    w0, w1 = column(r.wt[0:1, :], eye), column(r.wt[1:2, :], eye)
    hit0, hit1 = (e0 == lane_f), (e1 == lane_f)
    earlier = tri(tokens, True, True).astype(F32).astype(BF16)
    first_lane = lane_f * plane
    member = ((e0 >= first_lane) & (e0 < first_lane + plane)).astype(F32)
    named = (hit0.astype(F32) + hit1.astype(F32)).astype(BF16)
    before = mm(earlier, named)
    ahead_count = mm(earlier, member.astype(BF16))
    rank_group = jnp.sum(member * ahead_count, axis=1, keepdims=True)
    group = jnp.sum(member * lane_f, axis=1, keepdims=True)
    pick = (group * gcap + rank_group == lane_f).astype(F32).astype(BF16)
    r.pick[...] = pick
    for kind, ref in enumerate((r.mid, r.cot)):
        chosen = mm(pick, ref[...], TN).astype(BF16)
        for g in range(GROUPS):
            r.pack[g, kind] = chosen[g * gcap : (g + 1) * gcap]
    rank0 = jnp.sum(jnp.where(hit0, before, 0.0), axis=1, keepdims=True)
    rank1 = jnp.sum(jnp.where(hit1, before, 0.0), axis=1, keepdims=True)
    slot0 = (e0 - group * plane) * cap + rank0
    slot1 = (e1 - group * plane) * cap + rank1
    item = lax.broadcasted_iota(jnp.int32, (tokens, 8), 1)
    facts = jnp.where(item == 0, slot0, 0.0) + jnp.where(item == 1, slot1, 0.0)
    facts = split3(facts + jnp.where(item == 2, w0, 0.0) + jnp.where(item == 3, w1, 0.0))
    for g in range(GROUPS):
        some = ((group == g) & (rank_group == lane_f)).astype(F32).astype(BF16)
        r.pack_meta[g] = mm(facts[0], some, TN) + (mm(facts[1], some, TN) + mm(facts[2], some, TN))
    met(count)

    def z_copy(kind, step, there):
        target = lax.rem(z + step, GROUPS)
        return send(
            r.pack.at[target, kind], r.zbuf.at[there, kind], r.zs.at[kind, step], r.zr.at[kind, step],
            {"sp": target * plane + p},
        )

    def z_meta(step, there):
        target = lax.rem(z + step, GROUPS)
        return send(
            r.pack_meta.at[target], r.meta.at[there], r.zs.at[2, step], r.zr.at[2, step],
            {"sp": target * plane + p},
        )

    for step in STEPS[1:]:
        z_meta(step, z).start()
        for kind in range(2):
            z_copy(kind, step, z).start()
    r.meta[z] = r.pack_meta[z]
    for name in LATER:
        loads[name].start()

    def x_copy(kind, turn, step, there):
        target = lax.rem(p + step, plane)
        return send(
            r.wide.at[turn, kind, target], r.rows.at[kind, turn, core, there],
            r.xs.at[kind, turn, step], r.xr.at[kind, turn, step], {"sp": z * plane + target},
        )

    def own_copy(kind, turn):
        return pltpu.make_async_copy(
            r.wide.at[turn, kind, p], r.rows.at[kind, turn, core, p], r.own_sem.at[kind, turn]
        )

    def slot_table(turn):
        known = r.meta[source_of[turn]][:, :gcap]
        slot = lax.broadcasted_iota(jnp.int32, (slots, gcap), 0).astype(F32)
        return jnp.where(known[0:1] == slot, known[2:3], 0.0) + jnp.where(known[1:2] == slot, known[3:4], 0.0)

    def expand(kind, turn, ref):
        table = slot_table(turn)
        chosen = (table > 0).astype(F32).astype(BF16)
        if kind:
            scale = jnp.sum(table, axis=1, keepdims=True)
        chunk = 512
        for n in range(0, width, chunk):
            cols = slice(n, n + chunk)
            value = mm(chosen, ref[:, cols])
            if kind:
                value = scale * value
            r.wide[turn, kind, :, :, cols] = value.reshape(plane, cap, chunk).astype(BF16)
        loop(1, plane, lambda step: x_copy(kind, turn, step, p).start())
        own_copy(kind, turn).start()

    def receive(turn):
        step, source = STEPS[turn], source_of[turn]
        z_meta(step, source).wait_recv()
        for kind in range(2):
            z_copy(kind, step, source).wait_recv()
            expand(kind, turn, r.zbuf.at[source, kind])

    def forward(kind, turn, side):
        return send(
            r.rows.at[kind, turn, side], r.rows.at[kind, turn, side],
            r.fs.at[kind, turn], r.fr.at[kind, turn], {"tp": 1 - core},
        )

    def arrive(turn):
        for kind in range(2):
            own_copy(kind, turn).wait()
            loop(
                1, plane,
                lambda step: x_copy(kind, turn, step, lax.rem(p + plane - step, plane)).wait_recv(),
            )
            forward(kind, turn, core).start()

    def p_copy(turn):
        return send(r.part.at[turn, 1 - core], r.taken.at[turn], r.ps.at[turn], r.pr.at[turn], {"tp": 1 - core})

    def compute(turn):
        for kind in range(2):
            forward(kind, turn, 1 - core).wait_recv()
        many = 2 * slots

        def inner(n):
            cols = pl.ds(pl.multiple_of(n * 256, 256), 256)
            rows = r.rows[0, turn].reshape(many, width)
            pre_gate = mm(rows, r.gate[:, cols])
            pre_up = mm(rows, r.up[:, cols])
            back = mm(r.rows[1, turn].reshape(many, width), r.down[cols, :], NT)
            sig = jax.nn.sigmoid(pre_gate)
            swish = pre_gate * sig
            r.hidden[turn, :, cols] = (swish * pre_up).astype(BF16)
            r.back_up[turn, :, cols] = (back * swish).astype(BF16)
            r.back_gate[turn, :, cols] = (back * pre_up * (sig * (1.0 + pre_gate * (1.0 - sig)))).astype(BF16)

        loop(0, hide // 256, inner)

        def outer(n):
            cols = pl.ds(pl.multiple_of(n * 512, 512), 512)
            value = mm(r.back_gate[turn], r.gate[cols, :], NT) + mm(r.back_up[turn], r.up[cols, :], NT)
            r.part[turn, :, :, cols] = value.astype(BF16).reshape(2, slots, 512)

        loop(0, width // 512, outer)
        p_copy(turn).start()

    def e_copy(turn, step, there):
        target = lax.rem(p + step, plane)
        return send(
            r.result.at[turn, target], r.landed.at[turn, there], r.es.at[turn, step], r.er.at[turn, step],
            {"sp": z * plane + target},
        )

    def give_back(turn):
        p_copy(turn).wait_recv()
        value = r.part[turn, core].astype(F32) + r.taken[turn].astype(F32)
        r.result[turn] = value.astype(BF16).reshape(plane, cap, width)
        loop(1, plane, lambda step: e_copy(turn, step, p).start())
        r.landed[turn, p] = r.result[turn, p]

    def c_copy(turn, there):
        return send(
            r.comb.at[turn], r.home.at[there], r.cs.at[turn], r.cr.at[turn],
            {"sp": source_of[turn] * plane + p},
        )

    def combine(turn):
        loop(1, plane, lambda step: e_copy(turn, step, lax.rem(p + plane - step, plane)).wait_recv())
        chosen = (slot_table(turn) > 0).astype(F32).astype(BF16)
        value = mm(chosen, r.landed[turn].reshape(slots, width), TN).astype(BF16)
        if turn:
            r.comb[turn] = value
            c_copy(turn, z).start()
        else:
            r.home[z] = value

    expand(0, 0, r.pack.at[z, 0])
    expand(1, 0, r.pack.at[z, 1])

    for name in FIRST[4:]:
        loads[name].wait()
    low_b = low.astype(F32).astype(BF16)
    l3 = split3(r.ld[...])
    r.rl[...] = mm(low_b, l3[0]) + (mm(low_b, l3[1]) + mm(low_b, l3[2]))
    r.dec_mine[...] = jnp.exp(r.rl[length - 1 :, :])

    def d_copy(step, there):
        target = lax.rem(p + step, plane)
        return send(r.dec_mine, r.decs.at[there], r.ds.at[step], r.dr.at[step], {"sp": z * plane + target})

    def w_copy(step, there):
        target = lax.rem(z + step, GROUPS)
        return send(r.dec_plane, r.zdecs.at[there], r.ws.at[step], r.wr.at[step], {"sp": target * plane + p})

    loop(1, plane, lambda step: d_copy(step, p).start())
    r.decs[p] = r.dec_mine[...]

    def head(h):
        return head_parts(r.rl[...], r.q, r.k, h, mid_row)

    for h in range(heads):
        rl_h, mid, last, qs, kf = head(h)
        value = r.v[:, h * DV : (h + 1) * DV]
        to_end = split2(kf * jnp.exp(last - rl_h))
        total = mm2r(value, to_end, TN)
        r.total[:, h * DK : (h + 1) * DK] = total
        scatter_pieces(r.piece, total, h)
    scan = Scan(r.piece, r.got, r.lift, r.zgot, r.ready, r.inc, r.decs, r.zdecs, r.s1, r.r1, r.s2, r.r2, r.s5, r.r5, False)
    scan.start()

    arrive(0)
    loop(1, plane, lambda step: d_copy(step, lax.rem(p + plane - step, plane)).wait_recv())
    r.dec_plane[...] = lax.fori_loop(0, plane, lambda n, x: x * r.decs[n], jnp.ones(r.dec_mine.shape, F32))
    loop(1, GROUPS, lambda step: w_copy(step, z).start())
    scan.up()
    for name in LATER[:3]:
        loads[name].wait()
    compute(0)
    receive(1)
    give_back(0)
    receive(2)
    arrive(1)
    receive(3)
    compute(1)
    arrive(2)
    combine(0)
    give_back(1)
    compute(2)
    loop(1, GROUPS, lambda step: w_copy(step, lax.rem(z + GROUPS - step, GROUPS)).wait_recv())
    scan.down()
    arrive(3)
    give_back(2)
    compute(3)
    combine(1)
    give_back(3)
    scan.finish()

    pair = z + 1 - 2 * lax.rem(z, 2)
    across = lax.rem(z + 2, GROUPS)

    far = lax.rem(pair + 2, GROUPS)

    def n_copy(step, there):
        target = lax.rem(p + step, plane)
        return send(r.normed_rows, r.near.at[there], r.ns.at[step], r.nr.at[step], {"sp": z * plane + target})

    for h in range(heads):
        rl_h, mid, last, qs, kf = head(h)
        wide = slice(h * DV, (h + 1) * DV)
        up = split2(qs * jnp.exp(rl_h - mid))
        down = split2(kf * jnp.exp(mid - rl_h))
        score = jnp.where(low, mm3(up, down, NT), 0.0)
        r.score[h] = score
        decayed = split2(qs * jnp.exp(rl_h))
        state = r.inc[:, :, h * DK : (h + 1) * DK].reshape(DV, DK)
        raw = mm2l(split2(score), r.v[:, wide]) + mm3(decayed, split2(state), NT)
        inverse = lax.rsqrt(jnp.mean(raw * raw, axis=1, keepdims=True) + epsilon)
        out = raw * inverse
        r.normed[:, wide] = out
        r.normed_rows[:, wide] = out.astype(BF16)
        r.inv[:, h * 128 : (h + 1) * 128] = jnp.broadcast_to(inverse, (length, 128))
    loop(1, plane, lambda step: n_copy(step, p).start())
    r.near[p] = r.normed_rows[...]
    combine(2)
    all_rows = GROUPS * 2 * slots

    def gates(n):
        cols = pl.ds(pl.multiple_of(n * 256, 256), 256)
        rows = r.rows[0, :, :, :, :, cols].reshape(all_rows, 256)
        r.gate_out[cols, :] = mm(rows, r.back_gate[...].reshape(all_rows, hide), TN).astype(BF16)
        r.up_out[cols, :] = mm(rows, r.back_up[...].reshape(all_rows, hide), TN).astype(BF16)

    loop(0, width // 256, gates)
    combine(3)

    def downs(n):
        cols = pl.ds(pl.multiple_of(n * 256, 256), 256)
        hidden = r.hidden[:, :, cols].reshape(all_rows, 256)
        r.down_out[cols, :] = mm(hidden, r.rows[1].reshape(all_rows, width), TN).astype(BF16)

    loop(0, hide // 256, downs)

    for turn in range(1, GROUPS):
        c_copy(turn, lax.rem(z + STEPS[turn], GROUPS)).wait_recv()
    token = (
        r.cot[...].astype(F32) + mm(r.pick[...], r.home[...].reshape(GROUPS * gcap, width))
    ).astype(BF16)
    r.token[...] = token
    for other in range(plane):
        for g in range(GROUPS):
            start = (g * plane + other) * share
            r.cut[other, g] = token[:, start : start + share]
    r.both[core] = token

    def t_copy(side):
        return send(r.token, r.both.at[side], r.ts, r.tr, {"tp": 1 - core})

    def k_copy(step, there):
        target = lax.rem(p + step, plane)
        return send(
            r.cut.at[target], r.tok.at[there, core], r.ks.at[step], r.kr.at[step], {"sp": z * plane + target}
        )

    def k_pass(step, side):
        there = lax.rem(p + plane - step, plane)
        return send(
            r.tok.at[there, side], r.tok.at[there, side], r.js.at[step], r.jr.at[step], {"tp": 1 - core}
        )

    t_copy(core).start()
    loop(1, plane, lambda step: k_copy(step, p).start())
    r.tok[p, core] = r.cut[p]
    k_pass(0, core).start()
    t_copy(1 - core).wait_recv()

    loads["weight"].wait()
    for h in range(heads):
        wide = slice(h * DV, (h + 1) * DV)
        back = mm(r.both[...].reshape(length, width), r.weight[:, wide])
        normed = r.normed[:, wide]
        mean = jnp.mean(back * normed, axis=1, keepdims=True)
        inverse = r.inv[:, h * 128 : h * 128 + 1]
        value = inverse * (back - normed * mean)
        r.raw[:, wide] = value
        rl_h, mid, last, qs, kf = head(h)
        scatter_pieces(r.piece2, mm3(split2(value), split2(qs * jnp.exp(rl_h)), TN), h)
    scan2 = Scan(r.piece2, r.got2, r.lift2, r.zgot2, r.ready2, r.fut, r.decs, r.zdecs, r.s3, r.r3, r.s4, r.r4, r.s6, r.r6, True)
    scan2.start()

    half_cols = r.give.shape[3]

    def o_copy(n, part):
        aim = across if n == 2 else pair
        return send(
            r.give.at[n, part], r.take.at[n, part], r.os.at[n, part], r.orr.at[n, part], {"sp": aim * plane + p}
        )

    def terms(g):
        rows = plane * length
        return mm(r.tok[:, :, g].reshape(rows, share), r.near[...].reshape(rows, r.near.shape[2]), TN)

    for h in range(heads):
        rl_h, mid, last, qs, kf = head(h)
        cols = slice(h * DK, (h + 1) * DK)
        wide = slice(h * DV, (h + 1) * DV)
        back = split2(r.raw[:, wide])
        dots = split2(jnp.where(low, mm2l(back, r.v[:, wide], NT), 0.0))
        up_scale, down_scale = jnp.exp(rl_h - mid), jnp.exp(mid - rl_h)
        state = r.inc[:, :, cols].reshape(DV, DK)
        dq = up_scale * mm3(dots, split2(kf * down_scale)) + jnp.exp(rl_h) * mm3(back, split2(state))
        r.dq[:, cols] = (dq * DK ** (-0.5)).astype(BF16)
        r.run[0, :, cols] = down_scale * mm3(dots, split2(qs * up_scale), TN)
        r.run[1, :, cols] = qs * dq
        r.raw[:, wide] = mm3(split2(r.score[h]), back, TN)

    def k_arrive(step):
        k_copy(step, lax.rem(p + plane - step, plane)).wait_recv()
        k_pass(step, core).start()

    loop(1, plane, k_arrive)
    scan2.up()
    loop(0, plane, lambda step: k_pass(step, 1 - core).wait_recv())
    loop(1, plane, lambda step: n_copy(step, lax.rem(p + plane - step, plane)).wait_recv())
    for n, g in enumerate((far, pair)):
        value = terms(g).astype(BF16)
        for part in range(2):
            r.give[n, part] = value[:, part * half_cols : (part + 1) * half_cols]
            o_copy(n, part).start()
    r.own[1] = terms(across)
    r.own[0] = terms(z)
    for part in range(2):
        o_copy(0, part).wait_recv()
        cols = slice(part * half_cols, (part + 1) * half_cols)
        r.give[2, part] = (r.own[1, :, cols] + r.take[0, part].astype(F32)).astype(BF16)
        o_copy(2, part).start()
    scan2.down()
    scan2.finish()
    high_b = tri(length, False).astype(F32).astype(BF16)
    for h in range(heads):
        rl_h, mid, last, qs, kf = head(h)
        cols = slice(h * DK, (h + 1) * DK)
        wide = slice(h * DV, (h + 1) * DV)
        future = r.fut[:, :, cols].reshape(DV, DK)
        to_end = jnp.exp(last - rl_h)
        dk = r.run[0, :, cols] + to_end * mm2r(r.v[:, wide], split2(future))
        r.dk[:, cols] = dk.astype(BF16)
        r.dv[:, wide] = (r.raw[:, wide] + mm3(split2(kf * to_end), split2(future), NT)).astype(BF16)
        change = split3(r.run[1, :, cols] - kf * dk)
        later = mm(high_b, change[0]) + (mm(high_b, change[1]) + mm(high_b, change[2]))
        state = r.inc[:, :, cols].reshape(DV, DK).astype(F32)
        end = jnp.exp(last) * state + r.total[:, cols]
        r.da[:, cols] = later + jnp.sum(end * future.astype(F32), axis=0, keepdims=True)

    for part in range(2):
        o_copy(1, part).wait_recv()
        o_copy(2, part).wait_recv()
        cols = slice(part * half_cols, (part + 1) * half_cols)
        r.out[:, cols] = r.own[0, :, cols] + (r.take[1, part].astype(F32) + r.take[2, part].astype(F32))

    for n in range(3):
        for part in range(2):
            o_copy(n, part).wait_send()
    for step in STEPS[1:]:
        z_meta(step, z).wait_send()
        for kind in range(2):
            z_copy(kind, step, z).wait_send()
    for turn in range(GROUPS):
        for kind in range(2):
            loop(1, plane, lambda step: x_copy(kind, turn, step, p).wait_send())
            forward(kind, turn, core).wait_send()
        p_copy(turn).wait_send()
        loop(1, plane, lambda step: e_copy(turn, step, p).wait_send())
        if turn:
            c_copy(turn, z).wait_send()
    loop(1, plane, lambda step: d_copy(step, p).wait_send())
    loop(1, GROUPS, lambda step: w_copy(step, z).wait_send())

    loop(1, plane, lambda step: n_copy(step, p).wait_send())
    loop(1, plane, lambda step: k_copy(step, p).wait_send())
    loop(0, plane, lambda step: k_pass(step, core).wait_send())
    t_copy(core).wait_send()
    scan.settle()
    scan2.settle()


def whole(mid, cot, experts, weights, gate, up, down, weight, q, k, v, ld):
    count = lax.axis_size("sp")
    plane = count // GROUPS
    tokens, width = mid.shape
    cap = 4 * tokens // count
    slots = plane * cap
    gcap = slots // 2
    length, keys = q.shape
    heads = keys // DK
    values = v.shape[1]
    hide = gate.shape[1]
    share = width // count
    shape = jax.ShapeDtypeStruct
    dma = pltpu.SemaphoreType.DMA
    given = dict(
        mid=mid, cot=cot, ex=experts, wt=weights, q=q, k=k, v=v, ld=ld,
        gate=gate, up=up, down=down, weight=weight,
    )
    ins = {name + "_in": value for name, value in given.items()}
    outs = dict(
        gate_out=shape(gate.shape, BF16), up_out=shape(up.shape, BF16), down_out=shape(down.shape, BF16),
        out=shape((share, values), F32), dq=shape(q.shape, BF16), dk=shape(k.shape, BF16),
        dv=shape(v.shape, BF16), da=shape(q.shape, F32),
    )
    pieces = VMEM((plane, DV // plane, keys), F32)
    lifts = VMEM((DV // plane, keys), F32)
    zgots = VMEM((GROUPS, DV // plane, keys), F32)
    g3 = dma((2, GROUPS))
    scratch = {name: VMEM(value.shape, value.dtype) for name, value in given.items()}
    scratch |= dict(
        pick=VMEM((tokens, GROUPS * gcap), BF16),
        pack=VMEM((GROUPS, 2, gcap, width), BF16),
        pack_meta=VMEM((GROUPS, 8, 128), F32),
        meta=VMEM((GROUPS, 8, 128), F32),
        zbuf=VMEM((GROUPS, 2, gcap, width), BF16),
        wide=VMEM((GROUPS, 2, plane, cap, width), BF16),
        rows=VMEM((2, GROUPS, 2, plane, cap, width), BF16),
        hidden=VMEM((GROUPS, 2 * slots, hide), BF16),
        back_gate=VMEM((GROUPS, 2 * slots, hide), BF16),
        back_up=VMEM((GROUPS, 2 * slots, hide), BF16),
        part=VMEM((GROUPS, 2, slots, width), BF16),
        taken=VMEM((GROUPS, slots, width), BF16),
        result=VMEM((GROUPS, plane, cap, width), BF16),
        landed=VMEM((GROUPS, plane, cap, width), BF16),
        comb=VMEM((GROUPS, gcap, width), BF16),
        home=VMEM((GROUPS, gcap, width), BF16),
        rl=VMEM((length, keys), F32), dec_mine=VMEM((1, keys), F32), decs=VMEM((plane, 1, keys), F32), dec_plane=VMEM((1, keys), F32),
        zdecs=VMEM((GROUPS, 1, keys), F32),
        total=VMEM((DV, keys), F32), score=VMEM((heads, length, length), F32),
        normed=VMEM((length, values), F32), normed_rows=VMEM((length, values), BF16),
        inv=VMEM((length, heads * 128), F32), near=VMEM((plane, length, values), BF16),
        piece=pieces, got=pieces, ready=pieces, inc=pieces, lift=lifts, zgot=zgots, lift2=lifts, zgot2=zgots,
        piece2=pieces, got2=pieces, ready2=pieces, fut=pieces,
        token=VMEM((tokens, width), BF16), both=VMEM((2, tokens, width), BF16),
        cut=VMEM((plane, GROUPS, tokens, share), BF16), tok=VMEM((plane, 2, GROUPS, tokens, share), BF16),
        raw=VMEM((length, values), F32), run=VMEM((2, length, keys), F32),
        own=VMEM((2, share, values), F32), give=VMEM((3, 2, share, values // 2), BF16),
        take=VMEM((3, 2, share, values // 2), BF16),
        load_sem=dma((12,)), zs=dma((3, GROUPS)), zr=dma((3, GROUPS)), own_sem=g3, fs=g3, fr=g3,
        xs=dma((2, GROUPS, plane)), xr=dma((2, GROUPS, plane)),
        ps=dma((GROUPS,)), pr=dma((GROUPS,)), es=dma((GROUPS, plane)), er=dma((GROUPS, plane)),
        cs=dma((GROUPS,)), cr=dma((GROUPS,)), ds=dma((plane,)), dr=dma((plane,)),
        ws=dma((GROUPS,)), wr=dma((GROUPS,)),
        ns=dma((plane,)), nr=dma((plane,)), ks=dma((plane,)), kr=dma((plane,)), js=dma((plane,)), jr=dma((plane,)),
        ts=dma, tr=dma, os=dma((3, 2)), orr=dma((3, 2)),
        s1=dma((plane,)), r1=dma((plane,)), s2=dma((GROUPS,)), r2=dma((GROUPS,)), s5=dma((plane,)), r5=dma((plane,)),
        s3=dma((plane,)), r3=dma((plane,)), s4=dma((GROUPS,)), r4=dma((GROUPS,)), s6=dma((plane,)), r6=dma((plane,)),
    )
    vmem = pl.BlockSpec(memory_space=VMEM)
    return pl.pallas_call(
        functools.partial(whole_kernel, tuple(ins) + tuple(outs) + tuple(scratch)),
        out_shape=list(outs.values()),
        in_specs=[pl.BlockSpec(memory_space=pltpu.HBM)] * len(ins),
        out_specs=[vmem] * len(outs),
        scratch_shapes=list(scratch.values()),
        compiler_params=pltpu.CompilerParams(
            collective_id=0, has_side_effects=True, vmem_limit_bytes=LIMIT
        ),
        name="whole",
    )(*[pltpu.with_memory_space_constraint(x, pltpu.HBM) for x in ins.values()])


LIMIT = 44 * 2**20


def emit_kernel(number, *refs):
    copies = [
        pltpu.make_async_copy(refs[n], refs[number + n], refs[2 * number].at[n]) for n in range(number)
    ]
    for copy in copies:
        copy.start()
    for copy in copies:
        copy.wait()


def emit(values):
    number = len(values)
    return pl.pallas_call(
        functools.partial(emit_kernel, number),
        out_shape=[jax.ShapeDtypeStruct(x.shape, x.dtype) for x in values],
        in_specs=[pl.BlockSpec(memory_space=VMEM)] * number,
        out_specs=[pl.BlockSpec(memory_space=pl.ANY)] * number,
        scratch_shapes=[pltpu.SemaphoreType.DMA((number,))],
        compiler_params=pltpu.CompilerParams(vmem_limit_bytes=12 * 2**20),
        name="emit",
    )(*values)


def body(
    mid_rows,
    cotangent,
    route_experts,
    route_weights,
    gate_weight,
    up_weight,
    down_weight,
    out_weight,
    queries,
    key_rows,
    value_rows,
    log_decay,
):
    results = whole(
        mid_rows, cotangent, route_experts.T, route_weights.T, gate_weight[0], up_weight[0], down_weight[0],
        out_weight, queries, key_rows, value_rows, log_decay,
    )
    gate_grad, up_grad, down_grad, out_grad, dq, dk, dv, da = emit(results)
    return (gate_grad[None], up_grad[None], down_grad[None], out_grad, dq, dk, dv, da)


def solution(mesh):
    in_specs = (
        P(("sp", "tp"), None),
        P(("sp", "tp"), None),
        P(("sp", "tp"), None),
        P(("sp", "tp"), None),
        P("sp", None, "tp"),
        P("sp", None, "tp"),
        P("sp", "tp", None),
        P(None, "tp"),
        P("sp", "tp"),
        P("sp", "tp"),
        P("sp", "tp"),
        P("sp", "tp"),
    )
    out_specs = (
        P("sp", None, "tp"),
        P("sp", None, "tp"),
        P("sp", "tp", None),
        P("sp", "tp"),
        P("sp", "tp"),
        P("sp", "tp"),
        P("sp", "tp"),
        P("sp", "tp"),
    )
    return jax.shard_map(body, mesh=mesh, in_specs=in_specs, out_specs=out_specs, check_vma=False)
```
